512 devices in a mesh: sp: 64 (over z, y), tp: 8 (over x, core).
Axes of the slice: x: 4, y: 8, z: 8, core: 2. Of those that a mesh axis runs over, the one named last changes fastest.
Arguments:
- layer_source_rows: bfloat16 [24576, 2048], P(('sp', 'tp')), may hold values from -6 to 6
- entry_rescale_factor: bfloat16 [2048], replicated, may hold values from 0.099609375 to 1.8984375
- sliding_mixer_entry_matrix: bfloat16 [3, 2048, 1024], P(None, 'sp', 'tp'), may hold values from -0.125 to 0.125
- recurrent_mixer_entry_matrix: bfloat16 [2, 2048, 1024], P(None, 'sp', 'tp'), may hold values from -0.125 to 0.125
- latent_write_read_matrix: bfloat16 [2, 2048, 2048], P(None, 'sp', 'tp'), may hold values from -0.125 to 0.125
- timestep_matrix: bfloat16 [2048, 2, 16], P(None, None, 'tp'), may hold values from -0.125 to 0.125
- sliding_kernel_coefficients: bfloat16 [3, 1024], P(None, 'tp'), may hold values from -3.5 to 3.5
- recurrent_kernel_coefficients: bfloat16 [5, 1024], P(None, 'tp'), may hold values from -0.5 to 0.5
- latent_kernel_coefficients: bfloat16 [5, 2, 2048], P(None, None, 'tp'), may hold values from -0.5 to 0.5
- lane_forgetting_rate: float32 [2, 16], P(None, 'tp'), may hold values from 0 to 1
- spike_forgetting_rate: float32 [24576, 16], P('sp', 'tp'), may hold values from -2 to 0
- lane_rescale_factor: bfloat16 [1024], P('tp'), may hold values from 0.099609375 to 1.8984375
- sliding_mixer_exit_matrix: bfloat16 [1024, 2048], P('tp', 'sp'), may hold values from -0.125 to 0.125
- recurrent_mixer_exit_matrix: bfloat16 [1024, 2048], P('tp', 'sp'), may hold values from -0.125 to 0.125
Outputs:
- mixed_out: bfloat16 [24576, 2048], P(('sp', 'tp'))
The draws below stay inside these ranges and needn't reach their ends.
All inputs are finite; a program needn't handle non-finite values.
Results may differ from the reference program's by a relative error of at most 0.017.
Values may be sent and summed in bfloat16 or wider, within the bound.
A program may use at most 64 MiB of HBM per device.

```python
import jax
import jax.numpy as jnp
from jax import lax

D = 2048
CONV_CH = 1024
MIXER_LANES = 16
HEAD_DIM = 64
GROUPS = 16
STATE = 128
BLOCK = 128
CONV_TAPS = 3
SSD_TAPS = 5
TOK_DEV = 384
SSD_W = 1024
GROUP_HEADS = 1
SEQ_LENGTH = 24576
N_TP = 8


def draw_lane_forgetting_rate(key, part):
    flag_key = jax.random.fold_in(key, 11)
    level_key = jax.random.fold_in(key, 12)
    fraction = jax.random.uniform(level_key, (2, MIXER_LANES), jnp.float32)
    slow_rates = jnp.exp(jnp.log(0.1 / SEQ_LENGTH) + fraction * jnp.log(5.0))
    fast_rates = jnp.exp(jnp.log(0.01) + fraction * jnp.log(4.0))
    fast_flag = jax.random.randint(flag_key, (2, MIXER_LANES), 0, 2) == 1
    return jnp.where(fast_flag, fast_rates, slow_rates).astype(jnp.float32)


def draw_spike_forgetting_rate(key, part):
    level_key = jax.random.fold_in(key, 21)
    where_random_seed = jax.random.fold_in(key, 22)
    amount_random_seed = jax.random.fold_in(key, 23)
    blocks = SEQ_LENGTH // TOK_DEV
    fraction = jax.random.uniform(level_key, (blocks, MIXER_LANES), jnp.float32)
    levels = jnp.exp(jnp.log(0.1 / SEQ_LENGTH) + fraction * jnp.log(10.0))
    spread_amounts = jnp.repeat(levels, TOK_DEV, axis=0)
    spike_sites = jax.random.randint(where_random_seed, (3, MIXER_LANES), 0, SEQ_LENGTH)
    spike_amounts = jax.random.uniform(amount_random_seed, (3, MIXER_LANES), jnp.float32, 0.22, 0.5)
    sequence_indices = jnp.arange(SEQ_LENGTH)[:, None, None]
    spike_counts = (sequence_indices == spike_sites[None]).astype(jnp.float32)
    return (-spread_amounts - jnp.sum(spike_counts * spike_amounts[None], axis=1)).astype(jnp.float32)


def level_of(key, shape, pieces, least, high):
    loudness, own = 1.0, jax.random.fold_in(key, 6)
    for dim, shards_of in pieces:
        draws = jnp.exp(jax.random.uniform(jax.random.fold_in(own, dim), (shards_of,), jnp.float32, least / len(pieces), high / len(pieces)))
        loudness = loudness * jnp.repeat(draws, shape[dim] // shards_of).reshape([-1 if axis == dim else 1 for axis in range(len(shape))])
    return loudness


def gaussian(own_key, extent, deviation, reach, shards=(), kind=jnp.bfloat16):
    values = deviation * jax.random.normal(own_key, extent, jnp.float32)
    if shards:
        values = values * level_of(own_key, extent, shards, -0.22, 0.18)
    return jnp.clip(values, -reach, reach).astype(kind)


def setup_inputs(seed: int = 0) -> dict:
    streams_of = jax.random.split(jax.random.key(seed), 15)
    layer_source_rows = gaussian(streams_of[0], (SEQ_LENGTH, D), 1.0, 6.0, ((0, 512),))
    entry_rescale_factor = jnp.clip(1.0 + 0.18 * jax.random.normal(streams_of[1], (D,), jnp.float32), 0.099609375, 1.8984375).astype(jnp.bfloat16)
    sliding_mixer_entry_matrix = gaussian(streams_of[2], (3, D, CONV_CH), D ** -0.5, 0.125, ((1, 64), (2, 8)))
    recurrent_mixer_entry_matrix = gaussian(streams_of[3], (2, D, SSD_W), D ** -0.5, 0.125, ((1, 64), (2, 8)))
    latent_write_read_matrix = gaussian(streams_of[4], (2, D, GROUPS * STATE), D ** -0.5, 0.125, ((1, 64), (2, 8)))
    timestep_matrix = gaussian(streams_of[5], (D, 2, MIXER_LANES), D ** -0.5, 0.125, ((2, 8),))
    sliding_kernel_coefficients = gaussian(streams_of[6], (CONV_TAPS, CONV_CH), CONV_TAPS ** -0.5, 3.5, ((1, 8),))
    recurrent_kernel_coefficients = gaussian(streams_of[7], (SSD_TAPS, SSD_W), 0.09, 0.5, ((1, 8),))
    latent_kernel_coefficients = gaussian(streams_of[8], (SSD_TAPS, 2, GROUPS * STATE), 0.09, 0.5, ((2, 8),))
    lane_forgetting_rate = draw_lane_forgetting_rate(jax.random.fold_in(streams_of[14], 71), 0)
    spike_forgetting_rate = draw_spike_forgetting_rate(jax.random.fold_in(streams_of[14], 71), 0)
    lane_rescale_factor = jnp.clip(1.0 + 0.18 * jax.random.normal(streams_of[11], (SSD_W,), jnp.float32), 0.099609375, 1.8984375).astype(jnp.bfloat16)
    sliding_mixer_exit_matrix = gaussian(streams_of[12], (CONV_CH, D), (CONV_CH + SSD_W) ** -0.5, 0.125, ((0, 8), (1, 64)))
    recurrent_mixer_exit_matrix = gaussian(streams_of[13], (SSD_W, D), (CONV_CH + SSD_W) ** -0.5, 0.125, ((0, 8), (1, 64)))
    return dict(layer_source_rows=layer_source_rows, entry_rescale_factor=entry_rescale_factor, sliding_mixer_entry_matrix=sliding_mixer_entry_matrix, recurrent_mixer_entry_matrix=recurrent_mixer_entry_matrix, latent_write_read_matrix=latent_write_read_matrix, timestep_matrix=timestep_matrix, sliding_kernel_coefficients=sliding_kernel_coefficients, recurrent_kernel_coefficients=recurrent_kernel_coefficients, latent_kernel_coefficients=latent_kernel_coefficients, lane_forgetting_rate=lane_forgetting_rate, spike_forgetting_rate=spike_forgetting_rate, lane_rescale_factor=lane_rescale_factor, sliding_mixer_exit_matrix=sliding_mixer_exit_matrix, recurrent_mixer_exit_matrix=recurrent_mixer_exit_matrix)


epsilon = 1e-05

def centred_taps(values, tap_table):
    tap_count = tap_table.shape[0]
    half_width = tap_count // 2
    length = values.shape[0]
    padded = jnp.pad(values, ((half_width, half_width), (0, 0)))
    summed = jnp.zeros(values.shape, jnp.float32)
    for offset in range(tap_count):
        summed = summed + padded[offset:offset + length] * tap_table[offset].astype(jnp.float32)
    return summed

def project(normed, weight):
    return jnp.dot(normed, weight, preferred_element_type=jnp.float32).astype(jnp.bfloat16)

def direction_pass(ssd_x, keys_b, reads_c, timestep_deltas, forgetting_exponent):
    length = ssd_x.shape[0]
    blocks = length // BLOCK
    x_blocks = ssd_x.reshape(blocks, BLOCK, GROUPS, GROUP_HEADS, HEAD_DIM)
    b_blocks = keys_b.reshape(blocks, BLOCK, GROUPS, STATE)
    c_blocks = reads_c.reshape(blocks, BLOCK, GROUPS, STATE)
    d_blocks = timestep_deltas.reshape(blocks, BLOCK, GROUPS, GROUP_HEADS)
    l_blocks = forgetting_exponent.reshape(blocks, BLOCK, GROUPS, GROUP_HEADS)
    lower_mask = (jnp.arange(BLOCK)[:, None] >= jnp.arange(BLOCK)[None, :])[:, :, None, None]

    def one_block(carry_state, inputs):
        x_block, b_block, c_block, d_block, l_block = inputs
        running = jnp.cumsum(l_block, axis=0)
        log_gaps = jnp.where(lower_mask, running[:, None] - running[None, :], 0.0)
        decays = jnp.where(lower_mask, jnp.exp(log_gaps), 0.0)
        scores = jnp.einsum('tgn,sgn->tsg', c_block.astype(jnp.float32), b_block.astype(jnp.float32))
        weights = (scores[..., None] * decays * d_block[None]).astype(jnp.bfloat16)
        within = jnp.einsum('tsgr,sgrp->tgrp', weights.astype(jnp.float32), x_block.astype(jnp.float32))
        entering = lax.optimization_barrier(carry_state.astype(jnp.bfloat16)).astype(jnp.float32)
        carried = jnp.einsum('tgn,grpn->tgrp', c_block.astype(jnp.float32), entering) * jnp.exp(running)[..., None]
        to_end = jnp.exp(running[-1][None] - running) * d_block
        weighted = (x_block.astype(jnp.float32) * to_end[..., None]).astype(jnp.bfloat16)
        contribution = jnp.einsum('sgrp,sgn->grpn', weighted.astype(jnp.float32), b_block.astype(jnp.float32))
        next_state = carry_state * jnp.exp(running[-1])[..., None, None] + contribution
        return (next_state, within + carried)
    initial = jnp.zeros((GROUPS, GROUP_HEADS, HEAD_DIM, STATE), jnp.float32)
    final_state, outputs = lax.scan(one_block, initial, (x_blocks, b_blocks, c_blocks, d_blocks, l_blocks))
    return outputs.reshape(length, GROUPS, GROUP_HEADS, HEAD_DIM)

def reference(layer_source_rows, entry_rescale_factor, sliding_mixer_entry_matrix, recurrent_mixer_entry_matrix, latent_write_read_matrix, timestep_matrix, sliding_kernel_coefficients, recurrent_kernel_coefficients, latent_kernel_coefficients, lane_forgetting_rate, spike_forgetting_rate, lane_rescale_factor, sliding_mixer_exit_matrix, recurrent_mixer_exit_matrix):
    float_rows = layer_source_rows.astype(jnp.float32)
    normed = (float_rows * lax.rsqrt(lax.optimization_barrier(jnp.mean(float_rows * float_rows, axis=-1, keepdims=True)) + epsilon) * entry_rescale_factor.astype(jnp.float32)).astype(jnp.bfloat16)
    out_gate = project(normed, sliding_mixer_entry_matrix[0])
    in_gate = project(normed, sliding_mixer_entry_matrix[1])
    values = project(normed, sliding_mixer_entry_matrix[2])
    ssd_gate = project(normed, recurrent_mixer_entry_matrix[0])
    ssd_in = project(normed, recurrent_mixer_entry_matrix[1])
    inject = project(normed, latent_write_read_matrix[0])
    readout = project(normed, latent_write_read_matrix[1])
    raw_step = project(normed, timestep_matrix.reshape(timestep_matrix.shape[0], 2 * MIXER_LANES)).reshape(-1, 2, MIXER_LANES)
    gated_in = (in_gate.astype(jnp.float32) * values.astype(jnp.float32)).astype(jnp.bfloat16)
    y_conv = (out_gate.astype(jnp.float32) * centred_taps(gated_in.astype(jnp.float32), sliding_kernel_coefficients)).astype(jnp.bfloat16)
    joined = jnp.concatenate([ssd_in, inject, readout], axis=1).astype(jnp.float32)
    joined_taps = jnp.concatenate([recurrent_kernel_coefficients, latent_kernel_coefficients.reshape(latent_kernel_coefficients.shape[0], -1)], axis=1)
    mixed_ssd = jax.nn.silu(centred_taps(joined, joined_taps)).astype(jnp.bfloat16)
    length = layer_source_rows.shape[0]
    ssd_x = mixed_ssd[:, :SSD_W]
    keys_b = mixed_ssd[:, SSD_W:SSD_W + GROUPS * STATE]
    reads_c = mixed_ssd[:, SSD_W + GROUPS * STATE:]
    timestep_deltas = jax.nn.softplus(raw_step.astype(jnp.float32))
    forgetting_exponent = -timestep_deltas * lane_forgetting_rate.astype(jnp.float32)[None] + spike_forgetting_rate.astype(jnp.float32)[:, None, :]
    y_fwd = direction_pass(ssd_x, keys_b, reads_c, timestep_deltas[:, 0], forgetting_exponent[:, 0])
    y_bwd = jnp.flip(direction_pass(jnp.flip(ssd_x, 0), jnp.flip(keys_b, 0), jnp.flip(reads_c, 0), jnp.flip(timestep_deltas[:, 1], 0), jnp.flip(forgetting_exponent[:, 1], 0)), 0)
    gated_out = (y_fwd + y_bwd).reshape(length, SSD_W) * jax.nn.silu(ssd_gate.astype(jnp.float32))
    grouped = gated_out.reshape(length, GROUPS, GROUP_HEADS * HEAD_DIM)
    grouped = grouped * lax.rsqrt(lax.optimization_barrier(jnp.mean(grouped * grouped, axis=-1, keepdims=True)) + epsilon)
    y_ssd = (grouped.reshape(length, SSD_W) * lane_rescale_factor.astype(jnp.float32)).astype(jnp.bfloat16)
    conv_part = CONV_CH // N_TP
    ssd_part = SSD_W // N_TP
    summed = jnp.zeros((length, D), jnp.float32)
    for source in range(N_TP):
        partial_value = jnp.dot(y_conv[:, source * conv_part:(source + 1) * conv_part], sliding_mixer_exit_matrix[source * conv_part:(source + 1) * conv_part], preferred_element_type=jnp.float32)
        partial_value = partial_value + jnp.dot(y_ssd[:, source * ssd_part:(source + 1) * ssd_part], recurrent_mixer_exit_matrix[source * ssd_part:(source + 1) * ssd_part], preferred_element_type=jnp.float32)
        summed = summed + lax.optimization_barrier(partial_value.astype(jnp.bfloat16)).astype(jnp.float32)
    return summed.astype(jnp.bfloat16)
```

```python
import functools

import jax
import jax.numpy as jnp
from jax import lax
from jax.experimental import pallas as pl
from jax.experimental.pallas import tpu as pltpu
from jax.sharding import PartitionSpec as P

HEAD = 64
STATE = 128
CH = 128
EDGE = 16
EPS = 1e-05
BF = jnp.bfloat16
F32 = jnp.float32
MESH_IDS = pl.DeviceIdType.MESH


def wide(v):
    return v.astype(F32)


def dot_nt(a, b):
    return lax.dot_general(a, b, (((1,), (1,)), ((), ())), preferred_element_type=F32)


def dot_tn(a, b):
    return lax.dot_general(a, b, (((0,), (0,)), ((), ())), preferred_element_type=F32)


def silu(v):
    return v * jax.nn.sigmoid(v)


def softplus(v):
    return jnp.maximum(v, 0.0) + jnp.log1p(jnp.exp(-jnp.abs(v)))


def layer(
    n,
    tps,
    x_ref,
    gain_ref,
    slide_ref,
    rec_ref,
    lat_ref,
    step_ref,
    ctap_ref,
    xtap_ref,
    ltap_ref,
    rate_ref,
    spike_ref,
    lane_ref,
    cexit_ref,
    sexit_ref,
    out_ref,
    abuf,
    w1,
    w2,
    p1,
    p2,
    mixed,
    ycat,
    yacc,
    sb1,
    rb1,
    sb2,
    rb2,
    sb3,
    rb3,
    pre,
    prd,
    obf,
    prx,
    xsend,
    xrecv,
    s1,
    r1,
    s2,
    r2,
    ps,
    pr,
    asem,
    arem,
    hs,
    hr,
    es,
    er,
    os_,
    or_,
    xs,
    xr,
):
    rows = x_ref.shape[0]
    dim = x_ref.shape[1]
    nx = tps // 2
    length = rows * tps
    half = n // 2
    sl = HEAD // n
    ncol = os_.shape[0]
    wcol = dim // ncol
    sp = lax.axis_index("sp")
    tp = lax.axis_index("tp")
    z = sp // n
    y = sp % n
    cx = tp // 2
    core = tp % 2

    def remote(src, dst, ss, rs, zz, yy, tt):
        return pltpu.make_async_remote_copy(
            src_ref=src,
            dst_ref=dst,
            send_sem=ss,
            recv_sem=rs,
            device_id=(zz * n + yy, tt),
            device_id_type=MESH_IDS,
        )

    bar = pltpu.get_barrier_semaphore()

    def greet(s, t):
        pl.semaphore_signal(bar, inc=1, device_id=(s, t), device_id_type=MESH_IDS)

    for k in range(1, n):
        greet(z * n + (y + k) % n, tp)
        greet(((z + k) % n) * n + y, tp)
    for k in range(1, tps):
        greet(sp, (tp + k) % tps)
    greet((sp + 1) % (n * n), tp)
    greet((sp + n * n - 1) % (n * n), tp)

    xf = wide(x_ref[...])
    scale = lax.rsqrt(jnp.mean(xf * xf, axis=-1, keepdims=True) + EPS)
    own_rows = pl.ds(pl.multiple_of(EDGE + rows * tp, 16), rows)
    abuf[own_rows, :] = (xf * scale * wide(gain_ref[...])).astype(BF)

    @pl.when(sp == 0)
    def _():
        abuf[pl.ds(0, EDGE), :] = jnp.zeros((EDGE, dim), BF)

    @pl.when(sp == n * n - 1)
    def _():
        abuf[pl.ds(EDGE + length, EDGE), :] = jnp.zeros((EDGE, dim), BF)

    for h in range(2):
        cut = slice(16 * h, 16 * h + 16)
        w1[z, y, h, :, 0:128] = rec_ref[1, cut, :]
        w1[z, y, h, :, 128:384] = lat_ref[0, cut, :]
        w1[z, y, h, :, 384:640] = lat_ref[1, cut, :]
        w2[z, y, h, :, 0:128] = slide_ref[0, cut, :]
        w2[z, y, h, :, 128:256] = slide_ref[1, cut, :]
        w2[z, y, h, :, 256:384] = slide_ref[2, cut, :]
        w2[z, y, h, :, 384:512] = rec_ref[0, cut, :]
        w2[z, y, h, :, 512:640] = cexit_ref[cut, :]
        w2[z, y, h, :, 640:768] = sexit_ref[cut, :]

    pl.semaphore_wait(bar, 2 * (n - 1) + (tps - 1) + 2)

    def moved(h, phase, k):
        on_y = (h == 0) == (phase == 1)
        return (z, (y + k + n) % n) if on_y else ((z + k + n) % n, y)

    def piece(h, c, s, d):
        off = -((c + 1) // 2) if c % 2 else c // 2
        return place(h, off, s, d)

    def place(h, off, s, d):
        if h == 0:
            return (z - d * s + n) % n, (y + off + n) % n, 0
        return (z + off + n) % n, (y - d * s + n) % n, 1

    def ring_one(w, ss, rs, qs, qr, rnd):
        def first(h, c, nxt):
            d = 1 if nxt % 2 else -1
            ref = w.at[piece(h, c, 0, 1)]
            zz, yy = moved(h, 1, d)
            return remote(ref, ref, qs.at[rnd, h, nxt], qr.at[rnd, h, nxt], zz, yy, tp)

        def first_in(h, c):
            ref = w.at[piece(h, c, 0, 1)]
            return remote(ref, ref, qs.at[rnd, h, c], qr.at[rnd, h, c], z, y, tp)

        def second(h, off, c, s, di, d):
            ref = w.at[place(h, off, s, d)]
            zz, yy = moved(h, 2, d)
            return remote(ref, ref, ss.at[h, di, s, c], rs.at[h, di, s + 1, c], zz, yy, tp)

        def second_in(h, off, c, s, di, d):
            ref = w.at[place(h, off, s, d)]
            return remote(ref, ref, ss.at[h, di, 0, c], rs.at[h, di, s, c], z, y, tp)

        def offset(c):
            return jnp.where(c % 2 == 1, -((c + 1) // 2), c // 2)

        def start(c):
            for h in range(2):
                if c == 0:
                    first(h, 0, 1).start()
                    if n > 2:
                        first(h, 0, 2).start()
                else:
                    first_in(h, c).wait_recv()
                    if c + 2 < n:
                        first(h, c, c + 2).start()
                off = -((c + 1) // 2) if c % 2 else c // 2
                for di, d in ((0, 1), (1, -1)):
                    if half > 1 or di == c % 2:
                        second(h, off, c, 0, di, d).start()

        def pass_on(s, c):
            off = offset(c)
            for h in range(2):
                for di, d in ((0, 1), (1, -1)):
                    second_in(h, off, c, s, di, d).wait_recv()
                if s < half - 1:
                    for di, d in ((0, 1), (1, -1)):
                        second(h, off, c, s, di, d).start()
                else:
                    di = c % 2
                    second(h, off, c, s, di, 1 - 2 * di).start()

        def advance(lo, hi):
            while lo < hi:
                s, c = divmod(lo, n)
                if s == 0:
                    start(c)
                    lo += 1
                elif s < half:
                    stop = min(hi, (s + 1) * n)

                    @pl.loop(c, c + stop - lo)
                    def _(cc, s=s):
                        pass_on(s, cc)

                    lo = stop
                else:
                    stop = min(hi, (s + 1) * n)

                    @pl.loop(c, c + stop - lo)
                    def _(cc, s=s):
                        di = cc % 2
                        for h in range(2):
                            second_in(h, offset(cc), cc, s, di, 1 - 2 * di).wait_recv()

                    lo = stop

        def drain():
            for h in range(2):
                for c in range(1, n):
                    first_in(h, c).wait_send()

            @pl.loop(0, n)
            def _(c):
                off = offset(c)
                for h in range(2):
                    for s in range(half - 1):
                        for di, d in ((0, 1), (1, -1)):
                            second(h, off, c, s, di, d).wait_send()
                    di = c % 2
                    second(h, off, c, half - 1, di, 1 - 2 * di).wait_send()

        return advance, drain

    turns = (half + 1) * n
    ring1, drain1 = ring_one(w1, s1, r1, ps, pr, 0)
    ring2, drain2 = ring_one(w2, s2, r2, ps, pr, 1)

    def block(t):
        return abuf.at[pl.ds(pl.multiple_of(EDGE + rows * t, 16), rows), :]

    def a_out(k):
        return remote(block(tp), block(tp), asem.at[0, k], arem.at[0, k], z, y, ((cx + k) % nx) * 2 + core)

    def a_in(k):
        t = ((cx + nx - k) % nx) * 2 + core
        return remote(block(t), block(t), asem.at[0, k], arem.at[0, k], z, y, tp)

    def a_pair(k):
        t = ((cx + nx - k) % nx) * 2 + core
        return remote(block(t), block(t), asem.at[1, k], arem.at[1, k], z, y, cx * 2 + 1 - core)

    def a_pair_in(k):
        t = ((cx + nx - k) % nx) * 2 + 1 - core
        return remote(block(t), block(t), asem.at[1, k], arem.at[1, k], z, y, tp)

    before = abuf.at[pl.ds(0, EDGE), :]
    after = abuf.at[pl.ds(EDGE + length, EDGE), :]
    last_own = abuf.at[pl.ds(EDGE + length - EDGE, EDGE), :]
    first_own = abuf.at[pl.ds(EDGE, EDGE), :]
    down = (sp + n * n - 1) % (n * n)
    up = (sp + 1) % (n * n)
    far = tps - 1

    def edge_next():
        return remote(last_own, before, hs.at[0, 0], hr.at[0, 0], up // n, up % n, far)

    def edge_prev():
        return remote(first_own, after, hs.at[1, 0], hr.at[1, 0], down // n, down % n, 0)

    def edge_share(side, k):
        ref = (before, after)[side]
        return remote(ref, ref, hs.at[side, k], hr.at[side, k], z, y, ((far, 0)[side] + k) % tps)

    def edge_share_in(side, k):
        ref = (before, after)[side]
        return remote(ref, ref, hs.at[side, k], hr.at[side, k], z, y, tp)

    @pl.when((tp == far) & (sp < n * n - 1))
    def _():
        edge_next().start()

    @pl.when((tp == 0) & (sp > 0))
    def _():
        edge_prev().start()

    for k in range(1, nx):
        a_out(k).start()
    a_pair(0).start()

    ring1(0, n)

    @pl.when((tp == far) & (sp > 0))
    def _():
        edge_share_in(0, 0).wait_recv()
        for k in range(1, tps):
            edge_share(0, k).start()

    @pl.when((tp == 0) & (sp < n * n - 1))
    def _():
        edge_share_in(1, 0).wait_recv()
        for k in range(1, tps):
            edge_share(1, k).start()

    ring1(n, min(2 * n, half * n))
    for k in range(1, nx):
        if k != half_way(nx):
            a_in(k).wait_recv()
            a_pair(k).start()
    ring1(min(2 * n, half * n), half * n)
    if nx > 1:
        a_in(half_way(nx)).wait_recv()
        a_pair(half_way(nx)).start()
    ring2(0, 1)
    ring1(half * n, turns)
    for k in range(nx):
        a_pair_in(k).wait_recv()

    for side in range(2):
        edge_there = (sp > 0) if side == 0 else (sp < n * n - 1)
        for k in range(1, tps):

            @pl.when(edge_there & (tp == ((far, 0)[side] + k) % tps))
            def _(side=side, k=k):
                edge_share_in(side, k).wait_recv()

    tall = length + 2 * EDGE

    def project1(lo, hi):
        got = jnp.dot(abuf[...], w1[:, :, :, :, lo:hi].reshape(dim, hi - lo), preferred_element_type=F32)
        p1[:, lo:hi] = wide(got.astype(BF))

    tb = 128 if length % 128 == 0 else rows

    def mix(lo):
        if lo == 0:
            taps = wide(xtap_ref[...])
        else:
            at = lo - 128
            taps = wide(ltap_ref[:, at // 256, at % 256 : at % 256 + 128])
        for b in range(length // tb):
            acc = None
            for k in range(5):
                term = p1[EDGE - 2 + k + b * tb : EDGE - 2 + k + (b + 1) * tb, lo : lo + 128] * taps[k : k + 1, :]
                acc = term if acc is None else acc + term
            mixed[b * tb : (b + 1) * tb, lo : lo + 128] = silu(acc).astype(BF)

    project1(0, 256)
    ring2(1, 3)
    project1(256, 512)
    project1(512, 640)
    ring2(3, min(5, n))
    for j in range(5):
        mix(128 * j)

    steps = jnp.concatenate([step_ref[0], step_ref[1], jnp.zeros((12, dim), BF)], axis=0)
    raw = dot_nt(steps, abuf[EDGE : EDGE + length, :])[0:8]
    deltas = softplus(wide(raw.astype(BF)))
    spike = spike_ref[...]
    spikes = jnp.concatenate([spike, spike, jnp.zeros((4, length), F32)], axis=0)
    row_id = lax.broadcasted_iota(jnp.int32, (8, 1), 0)
    rates = jnp.zeros((8, 1), F32)
    for k in range(4):
        rates = jnp.where(row_id == k, rate_ref[k // 2, k % 2], rates)
    logs = spikes - deltas * rates
    logs = jnp.where(row_id < 4, logs, 0.0)
    lane = lax.broadcasted_iota(jnp.int32, (8, length), 1)
    fsum = logs
    bsum = logs
    shift = 1
    while shift < length:
        fsum = fsum + jnp.where(lane >= shift, pltpu.roll(fsum, shift, axis=1), 0.0)
        bsum = bsum + jnp.where(lane < length - shift, pltpu.roll(bsum, length - shift, axis=1), 0.0)
        shift *= 2
    run = jnp.where(row_id < 2, fsum, bsum)
    total = jnp.where(row_id < 2, fsum[:, length - 1 : length], bsum[:, 0:1])
    weight = jnp.exp(total - run) * deltas
    turned = jnp.concatenate([run, weight, jnp.exp(run), jnp.zeros((CH - 24, length), F32)], axis=0).T

    low = lax.broadcasted_iota(jnp.int32, (length, CH), 1) < HEAD
    xs_all = wide(mixed[:, 0:128])
    states = []
    for d in range(2):
        w_d = jnp.where(low, turned[:, 8 + 2 * d : 9 + 2 * d], turned[:, 9 + 2 * d : 10 + 2 * d])
        xw = (xs_all * w_d).astype(BF)
        for h in range(2):
            full = dot_tn(xw, mixed[:, 128 + 128 * h : 256 + 128 * h])
            states.append(full[HEAD * h : HEAD * h + HEAD, :])
    decay = jnp.broadcast_to(jnp.exp(total), (8, STATE))

    def packed(parts, dec):
        high = dec.astype(BF)
        rest = dec - wide(high)
        return jnp.concatenate([*parts, wide(high), rest], axis=0).astype(BF)

    for j in range(n):
        got = packed([s[sl * j : sl * j + sl, :] for s in states], decay)
        sb1[j] = got
    rb1[y] = sb1[y]

    def e1(k):
        yy = (y + k) % n
        return remote(sb1.at[yy], rb1.at[y], es.at[0, k], er.at[0, k], z, yy, tp)

    def e2(k):
        return remote(sb2, rb2.at[z], es.at[1, k], er.at[1, k], (z + k) % n, y, tp)

    def e3(k):
        yy = (y + k) % n
        return remote(sb3.at[yy], rb3.at[y], es.at[2, k], er.at[2, k], z, yy, tp)

    def e_in(which, k):
        if which == 0:
            ref = rb1.at[(y - k + n) % n]
        elif which == 1:
            ref = rb2.at[(z - k + n) % n]
        else:
            ref = rb3.at[(y - k + n) % n]
        return remote(ref, ref, es.at[which, k], er.at[which, k], z, y, tp)

    for k in range(1, n):
        e1(k).start()

    runs = [run[k : k + 1, :] for k in range(4)]
    dels = [deltas[k : k + 1, :] for k in range(4)]

    def within(h, b):
        scores = dot_nt(
            mixed[b * tb : (b + 1) * tb, 384 + 128 * h : 512 + 128 * h],
            mixed[:, 128 + 128 * h : 256 + 128 * h],
        )
        t_id = lax.broadcasted_iota(jnp.int32, (tb, length), 0) + b * tb
        s_id = lax.broadcasted_iota(jnp.int32, (tb, length), 1)
        part = turned[b * tb : (b + 1) * tb, :]
        gap_f = part[:, h : h + 1] - runs[h]
        gap_b = part[:, 2 + h : 3 + h] - runs[2 + h]
        factor = jnp.where(s_id < t_id, dels[h], jnp.where(s_id > t_id, dels[2 + h], dels[h] + dels[2 + h]))
        decays = jnp.exp(jnp.where(s_id < t_id, gap_f, jnp.where(s_id > t_id, gap_b, 0.0)))
        weights = (scores * decays * factor).astype(BF)
        keep = (lax.broadcasted_iota(jnp.int32, (length, CH), 1) // HEAD) == h
        x_h = jnp.where(keep, xs_all, 0.0).astype(BF)
        got = jnp.dot(weights, x_h, preferred_element_type=F32)
        at = slice(b * tb, (b + 1) * tb)
        yacc[at, :] = got if h == 0 else yacc[at, :] + got

    spots = [(h, b) for h in range(2) for b in range(length // tb)]
    at_turn = min(5, n)
    for i, (h, b) in enumerate(spots):
        within(h, b)
        to = min(n, at_turn + 1)
        ring2(at_turn, to)
        at_turn = to

    for k in range(1, n):
        e_in(0, k).wait_recv()

    def opened(ref):
        blk = wide(ref[...])
        parts = [blk[sl * q : sl * q + sl, :] for q in range(4)]
        base = 4 * sl
        decs = [blk[base + q : base + q + 1, :] + blk[base + 8 + q : base + 9 + q, :] for q in range(4)]
        return parts, decs

    carry = [jnp.zeros((sl, STATE), F32) for _ in range(4)]
    prod = [jnp.ones((1, STATE), F32) for _ in range(4)]
    for j in range(n):
        for q in range(4):
            jj = j if q < 2 else n - 1 - j
            blk = wide(rb1[jj])
            pre[jj, sl * q : sl * q + sl, :] = carry[q]
            prd[jj, q : q + 1, :] = prod[q]
            dec = blk[4 * sl + q : 4 * sl + q + 1, :] + blk[4 * sl + 8 + q : 4 * sl + 9 + q, :]
            carry[q] = carry[q] * dec + blk[sl * q : sl * q + sl, :]
            prod[q] = prod[q] * dec
    prods = jnp.concatenate([*prod, jnp.zeros((4, STATE), F32)], axis=0)
    sb2[...] = packed(carry, prods)
    for k in range(1, n):
        e2(k).start()
    to = min(2 * n, half * n)
    ring2(at_turn, max(at_turn, to))
    at_turn = max(at_turn, to)
    for k in range(1, n):
        e_in(1, k).wait_recv()
    entry = [jnp.zeros((sl, STATE), F32) for _ in range(4)]
    for j in range(n):
        for q in range(4):
            jj = j if q < 2 else n - 1 - j
            blk = wide(rb2[jj])
            dec = blk[4 * sl + q : 4 * sl + q + 1, :] + blk[4 * sl + 8 + q : 4 * sl + 9 + q, :]
            ahead = (jj < z) if q < 2 else (jj > z)
            entry[q] = jnp.where(ahead, entry[q] * dec + blk[sl * q : sl * q + sl, :], entry[q])
    for j in range(n):
        parts = [entry[q] * prd[j, q : q + 1, :] + pre[j, sl * q : sl * q + sl, :] for q in range(4)]
        sb3[j] = jnp.concatenate(parts, axis=0).astype(BF)
    rb3[y] = sb3[y]
    for k in range(1, n):
        e3(k).start()

    ring2(at_turn, half * n)
    ring2(half * n, turns)

    def project2(lo, hi):
        got = jnp.dot(abuf[...], w2[:, :, :, :, lo:hi].reshape(dim, hi - lo), preferred_element_type=F32)
        p2[:, lo:hi] = wide(got.astype(BF))

    project2(0, 256)
    project2(256, 512)
    p2[:, 128:256] = wide((p2[:, 128:256] * p2[:, 256:384]).astype(BF))
    ctaps = wide(ctap_ref[...])
    for b in range(length // tb):
        acc = None
        for k in range(3):
            term = p2[EDGE - 1 + k + b * tb : EDGE - 1 + k + (b + 1) * tb, 128:256] * ctaps[k : k + 1, :]
            acc = term if acc is None else acc + term
        ycat[b * tb : (b + 1) * tb, 0:128] = (p2[EDGE + b * tb : EDGE + (b + 1) * tb, 0:128] * acc).astype(BF)

    for k in range(1, n):
        e_in(2, k).wait_recv()
    blocks = [wide(rb3[j]) for j in range(n)]
    arrived = [
        jnp.concatenate([blk[sl * q : sl * q + sl, :] for blk in blocks], axis=0).astype(BF) for q in range(4)
    ]
    none = jnp.zeros((HEAD, STATE), BF)
    y_all = yacc[...]
    for d in range(2):
        top = jnp.concatenate([arrived[2 * d], none], axis=1)
        bottom = jnp.concatenate([none, arrived[2 * d + 1]], axis=1)
        into = dot_nt(mixed[:, 384:640], jnp.concatenate([top, bottom], axis=0))
        grow = jnp.where(low, turned[:, 16 + 2 * d : 17 + 2 * d], turned[:, 17 + 2 * d : 18 + 2 * d])
        y_all = y_all + into * grow
    g = y_all * silu(p2[EDGE : EDGE + length, 384:512])
    sq = g * g
    mean0 = jnp.sum(jnp.where(low, sq, 0.0), axis=-1, keepdims=True) / HEAD
    mean1 = jnp.sum(jnp.where(low, 0.0, sq), axis=-1, keepdims=True) / HEAD
    inv = jnp.where(low, lax.rsqrt(mean0 + EPS), lax.rsqrt(mean1 + EPS))
    ycat[:, 128:256] = (g * inv * wide(lane_ref[...])).astype(BF)

    def to_pair(c):
        cols = slice(c * wcol, (c + 1) * wcol)
        return remote(
            obf.at[:, 1 - core, :, cols], prx.at[:, :, cols], os_.at[c], or_.at[c], z, y, cx * 2 + 1 - core
        )

    def to_owner(c, k):
        cols = slice(c * wcol, (c + 1) * wcol)
        xx = (cx + k) % nx
        return remote(
            xsend.at[xx, :, cols], xrecv.at[k, :, cols], xs.at[c, k], xr.at[c, k], z, y, xx * 2 + core
        )

    exits = w2[:, :, :, :, 512:768].reshape(dim, 2 * CH)
    for c in range(ncol):
        cols = slice(c * wcol, (c + 1) * wcol)
        got = dot_nt(ycat[...], exits[c * wcol : (c + 1) * wcol, :])
        obf[:, :, :, cols] = got.astype(BF).reshape(nx, 2, rows, wcol)
        to_pair(c).start()
    for c in range(ncol):
        cols = slice(c * wcol, (c + 1) * wcol)
        to_pair(c).wait_recv()
        for xx in range(nx):
            both = wide(obf[xx, core, :, cols]) + wide(prx[xx, :, cols])
            xsend[xx, :, cols] = both.astype(BF)
        for k in range(1, nx):
            to_owner(c, k).start()
    drain1()
    drain2()
    for c in range(ncol):
        cols = slice(c * wcol, (c + 1) * wcol)
        both = wide(obf[cx, core, :, cols]) + wide(prx[cx, :, cols])
        for k in range(1, nx):
            to_owner(c, k).wait_recv()
            both = both + wide(xrecv[k, :, cols])
        out_ref[:, cols] = both.astype(BF)

    for c in range(ncol):
        to_pair(c).wait_send()
        for k in range(1, nx):
            to_owner(c, k).wait_send()
    for k in range(1, n):
        e1(k).wait_send()
        e2(k).wait_send()
        e3(k).wait_send()
    for k in range(1, nx):
        a_out(k).wait_send()
    for k in range(nx):
        a_pair(k).wait_send()

    @pl.when((tp == far) & (sp < n * n - 1))
    def _():
        edge_next().wait_send()

    @pl.when((tp == 0) & (sp > 0))
    def _():
        edge_prev().wait_send()

    @pl.when((tp == far) & (sp > 0))
    def _():
        for k in range(1, tps):
            edge_share(0, k).wait_send()

    @pl.when((tp == 0) & (sp < n * n - 1))
    def _():
        for k in range(1, tps):
            edge_share(1, k).wait_send()


def half_way(nx):
    return nx // 2


def run_layer(n, tps, ncol, *args):
    (
        x,
        gain,
        slide,
        rec,
        lat,
        step,
        ctap,
        xtap,
        ltap,
        rate,
        spike,
        lane,
        cexit,
        sexit,
    ) = args
    rows, dim = x.shape
    length = rows * tps
    tall = length + 2 * EDGE
    nx = tps // 2
    half = n // 2
    sl = HEAD // n
    vm = pltpu.VMEM
    dma = pltpu.SemaphoreType.DMA
    vmem = pl.BlockSpec(memory_space=pltpu.VMEM)
    specs = [vmem] * 14
    specs[9] = pl.BlockSpec(memory_space=pltpu.SMEM)
    return pl.pallas_call(
        functools.partial(layer, n, tps),
        out_shape=jax.ShapeDtypeStruct((rows, dim), BF),
        in_specs=specs,
        out_specs=vmem,
        scratch_shapes=[
            vm((tall, dim), BF),
            vm((n, n, 2, 16, 640), BF),
            vm((n, n, 2, 16, 768), BF),
            vm((tall, 640), F32),
            vm((tall, 512), F32),
            vm((length, 640), BF),
            vm((length, 256), BF),
            vm((length, 128), F32),
            vm((n, 4 * sl + 16, STATE), BF),
            vm((n, 4 * sl + 16, STATE), BF),
            vm((4 * sl + 16, STATE), BF),
            vm((n, 4 * sl + 16, STATE), BF),
            vm((n, 4 * sl, STATE), BF),
            vm((n, 4 * sl, STATE), BF),
            vm((n, 4 * sl, STATE), F32),
            vm((n, 8, STATE), F32),
            vm((nx, 2, rows, dim), BF),
            vm((nx, rows, dim), BF),
            vm((nx, rows, dim), BF),
            vm((nx, rows, dim), BF),
            dma((2, 2, half + 1, n)),
            dma((2, 2, half + 1, n)),
            dma((2, 2, half + 1, n)),
            dma((2, 2, half + 1, n)),
            dma((2, 2, n)),
            dma((2, 2, n)),
            dma((2, nx)),
            dma((2, nx)),
            dma((2, tps)),
            dma((2, tps)),
            dma((3, n)),
            dma((3, n)),
            dma((ncol,)),
            dma((ncol,)),
            dma((ncol, nx)),
            dma((ncol, nx)),
        ],
        compiler_params=pltpu.CompilerParams(
            collective_id=0, has_side_effects=True, vmem_limit_bytes=60 * 1024 * 1024
        ),
        name="layer",
    )(
        x,
        gain.reshape(1, dim),
        slide,
        rec,
        lat,
        step.transpose(1, 2, 0),
        ctap,
        xtap,
        ltap,
        rate,
        spike.T,
        lane.reshape(1, CH),
        cexit.T,
        sexit.T,
    )


def solution(mesh):
    n = 8 if mesh.shape["sp"] == 64 else int(round(mesh.shape["sp"] ** 0.5))
    sp_tp = ("sp", "tp")
    return jax.shard_map(
        functools.partial(run_layer, n, mesh.shape["tp"], 4),
        mesh=mesh,
        in_specs=(
            P(sp_tp, None),
            P(),
            P(None, "sp", "tp"),
            P(None, "sp", "tp"),
            P(None, "sp", "tp"),
            P(None, None, "tp"),
            P(None, "tp"),
            P(None, "tp"),
            P(None, None, "tp"),
            P(None, "tp"),
            P("sp", "tp"),
            P("tp"),
            P("tp", "sp"),
            P("tp", "sp"),
        ),
        out_specs=P(sp_tp, None),
        check_vma=False,
    )
```

```python
import functools

import jax
import jax.numpy as jnp
from jax import lax
from jax.experimental import pallas as pl
from jax.experimental.pallas import tpu as pltpu
from jax.sharding import PartitionSpec as P

HEAD = 64
STATE = 128
CH = 128
EDGE = 16
EPS = 1e-05
BF = jnp.bfloat16
F32 = jnp.float32
MESH_IDS = pl.DeviceIdType.MESH


def wide(v):
    return v.astype(F32)


def dot_nt(a, b):
    return lax.dot_general(a, b, (((1,), (1,)), ((), ())), preferred_element_type=F32)


def dot_tn(a, b):
    return lax.dot_general(a, b, (((0,), (0,)), ((), ())), preferred_element_type=F32)


def silu(v):
    return v * jax.nn.sigmoid(v)


def softplus(v):
    return jnp.maximum(v, 0.0) + jnp.log1p(jnp.exp(-jnp.abs(v)))


def layer(
    n,
    tps,
    x_hbm,
    gain_hbm,
    slide_hbm,
    rec_hbm,
    lat_hbm,
    step_hbm,
    ctap_hbm,
    xtap_hbm,
    ltap_hbm,
    rate_hbm,
    spike_hbm,
    lane_hbm,
    cexit_hbm,
    sexit_hbm,
    out_ref,
    abuf,
    w1,
    w2,
    p1,
    p2,
    mixed,
    ycat,
    yacc,
    sb1,
    rb1,
    sb2,
    rb2,
    sb3,
    rb3,
    pre,
    prd,
    obf,
    prx,
    xsend,
    xrecv,
    s1,
    r1,
    s2,
    r2,
    ps,
    pr,
    asem,
    arem,
    hs,
    hr,
    es,
    er,
    os_,
    or_,
    xs,
    xr,
    x_ref,
    gain_ref,
    slide_ref,
    rec_ref,
    lat_ref,
    step_ref,
    ctap_ref,
    xtap_ref,
    ltap_ref,
    rate_ref,
    spike_ref,
    lane_ref,
    cexit_ref,
    sexit_ref,
    ins,
):
    rows = x_ref.shape[0]
    dim = x_ref.shape[1]
    nx = tps // 2
    length = rows * tps
    half = n // 2
    sl = HEAD // n
    ncol = os_.shape[0]
    wcol = dim // ncol
    sp = lax.axis_index("sp")
    tp = lax.axis_index("tp")
    z = sp // n
    y = sp % n
    cx = tp // 2
    core = tp % 2

    def remote(src, dst, ss, rs, zz, yy, tt):
        return pltpu.make_async_remote_copy(
            src_ref=src,
            dst_ref=dst,
            send_sem=ss,
            recv_sem=rs,
            device_id=(zz * n + yy, tt),
            device_id_type=MESH_IDS,
        )

    given = (
        (x_hbm, x_ref),
        (gain_hbm, gain_ref),
        (slide_hbm, slide_ref),
        (rec_hbm, rec_ref),
        (lat_hbm, lat_ref),
        (step_hbm, step_ref),
        (ctap_hbm, ctap_ref),
        (xtap_hbm, xtap_ref),
        (ltap_hbm, ltap_ref),
        (rate_hbm, rate_ref),
        (spike_hbm, spike_ref),
        (lane_hbm, lane_ref),
        (cexit_hbm, cexit_ref),
        (sexit_hbm, sexit_ref),
    )
    loads = [pltpu.make_async_copy(src, dst, ins.at[i]) for i, (src, dst) in enumerate(given)]
    for load in loads:
        load.start()

    bar = pltpu.get_barrier_semaphore()

    def greet(s, t):
        pl.semaphore_signal(bar, inc=1, device_id=(s, t), device_id_type=MESH_IDS)

    for k in range(1, n):
        greet(z * n + (y + k) % n, tp)
        greet(((z + k) % n) * n + y, tp)
    for k in range(1, tps):
        greet(sp, (tp + k) % tps)
    greet((sp + 1) % (n * n), tp)
    greet((sp + n * n - 1) % (n * n), tp)

    for load in loads:
        load.wait()
    xf = wide(x_ref[...])
    scale = lax.rsqrt(jnp.mean(xf * xf, axis=-1, keepdims=True) + EPS)
    own_rows = pl.ds(pl.multiple_of(EDGE + rows * tp, 16), rows)
    gains = wide(gain_ref[...])
    for j in range(dim // 128):
        cols = slice(128 * j, 128 * j + 128)
        abuf[own_rows, cols] = (xf[:, cols] * scale * gains[j : j + 1, :]).astype(BF)

    @pl.when(sp == 0)
    def _():
        abuf[pl.ds(0, EDGE), :] = jnp.zeros((EDGE, dim), BF)

    @pl.when(sp == n * n - 1)
    def _():
        abuf[pl.ds(EDGE + length, EDGE), :] = jnp.zeros((EDGE, dim), BF)

    for h in range(2):
        cut = slice(16 * h, 16 * h + 16)
        w1[z, y, h, :, 0:128] = rec_ref[1, cut, :]
        w1[z, y, h, :, 128:384] = lat_ref[0, cut, :]
        w1[z, y, h, :, 384:640] = lat_ref[1, cut, :]
        w2[z, y, h, :, 0:128] = slide_ref[0, cut, :]
        w2[z, y, h, :, 128:256] = slide_ref[1, cut, :]
        w2[z, y, h, :, 256:384] = slide_ref[2, cut, :]
        w2[z, y, h, :, 384:512] = rec_ref[0, cut, :]
        w2[z, y, h, :, 512:640] = cexit_ref[cut, :]
        w2[z, y, h, :, 640:768] = sexit_ref[cut, :]

    pl.semaphore_wait(bar, 2 * (n - 1) + (tps - 1) + 2)

    def moved(h, phase, k):
        on_y = (h == 0) == (phase == 1)
        return (z, (y + k + n) % n) if on_y else ((z + k + n) % n, y)

    def piece(h, c, s, d):
        off = -((c + 1) // 2) if c % 2 else c // 2
        return place(h, off, s, d)

    def place(h, off, s, d):
        if h == 0:
            return (z - d * s + n) % n, (y + off + n) % n, 0
        return (z + off + n) % n, (y - d * s + n) % n, 1

    def ring_one(w, ss, rs, qs, qr, rnd, straight):
        def first(h, c, nxt):
            d = 1 if nxt % 2 else -1
            ref = w.at[piece(h, c, 0, 1)]
            zz, yy = moved(h, 1, d)
            return remote(ref, ref, qs.at[rnd, h, nxt], qr.at[rnd, h, nxt], zz, yy, tp)

        def first_in(h, c):
            ref = w.at[piece(h, c, 0, 1)]
            return remote(ref, ref, qs.at[rnd, h, c], qr.at[rnd, h, c], z, y, tp)

        def second(h, off, c, s, di, d):
            ref = w.at[place(h, off, s, d)]
            zz, yy = moved(h, 2, d)
            return remote(ref, ref, ss.at[h, di, s, c], rs.at[h, di, s + 1, c], zz, yy, tp)

        def second_in(h, off, c, s, di, d):
            ref = w.at[place(h, off, s, d)]
            return remote(ref, ref, ss.at[h, di, 0, c], rs.at[h, di, s, c], z, y, tp)

        def offset(c):
            return jnp.where(c % 2 == 1, -((c + 1) // 2), c // 2)

        def direct(h, c):
            d = (c + 1) // 2 if c % 2 else -(c // 2)
            ref = w.at[piece(h, 0, 0, 1)]
            zz, yy = moved(h, 1, d)
            return remote(ref, ref, qs.at[rnd, h, c], qr.at[rnd, h, c], zz, yy, tp)

        def spread(lo, hi):
            for c in range(lo, hi):
                for h in range(2):
                    direct(h, c).start()

        def lead(lo, hi):
            for c in range(lo, hi):
                for h in range(2):
                    if c == 0:
                        first(h, 0, 1).start()
                        if n > 2:
                            first(h, 0, 2).start()
                    else:
                        first_in(h, c).wait_recv()
                        if c + 2 < n:
                            first(h, c, c + 2).start()

        def start(c):
            for h in range(2):
                if straight and c > 0:
                    first_in(h, c).wait_recv()
                off = -((c + 1) // 2) if c % 2 else c // 2
                for di, d in ((0, 1), (1, -1)):
                    if half > 1 or di == c % 2:
                        second(h, off, c, 0, di, d).start()

        def pass_on(s, c):
            off = offset(c)
            for h in range(2):
                for di, d in ((0, 1), (1, -1)):
                    second_in(h, off, c, s, di, d).wait_recv()
                if s < half - 1:
                    for di, d in ((0, 1), (1, -1)):
                        second(h, off, c, s, di, d).start()
                else:
                    di = c % 2
                    second(h, off, c, s, di, 1 - 2 * di).start()

        def advance(lo, hi):
            while lo < hi:
                s, c = divmod(lo, n)
                if s == 0:
                    start(c)
                    lo += 1
                elif s < half:
                    stop = min(hi, (s + 1) * n)

                    @pl.loop(c, c + stop - lo)
                    def _(cc, s=s):
                        pass_on(s, cc)

                    lo = stop
                else:
                    stop = min(hi, (s + 1) * n)

                    @pl.loop(c, c + stop - lo)
                    def _(cc, s=s):
                        di = cc % 2
                        for h in range(2):
                            second_in(h, offset(cc), cc, s, di, 1 - 2 * di).wait_recv()

                    lo = stop

        def drain():
            for h in range(2):
                for c in range(1, n):
                    first_in(h, c).wait_send()

            @pl.loop(0, n)
            def _(c):
                off = offset(c)
                for h in range(2):
                    for s in range(half - 1):
                        for di, d in ((0, 1), (1, -1)):
                            second(h, off, c, s, di, d).wait_send()
                    di = c % 2
                    second(h, off, c, half - 1, di, 1 - 2 * di).wait_send()

        return advance, drain, spread, lead

    turns = (half + 1) * n
    ring1, drain1, spread1, _ = ring_one(w1, s1, r1, ps, pr, 0, True)
    ring2, drain2, _, lead2 = ring_one(w2, s2, r2, ps, pr, 1, False)

    def block(t):
        return abuf.at[pl.ds(pl.multiple_of(EDGE + rows * t, 16), rows), :]

    def a_out(k):
        return remote(block(tp), block(tp), asem.at[0, k], arem.at[0, k], z, y, ((cx + k) % nx) * 2 + core)

    def a_in(k):
        t = ((cx + nx - k) % nx) * 2 + core
        return remote(block(t), block(t), asem.at[0, k], arem.at[0, k], z, y, tp)

    def a_pair(k):
        t = ((cx + nx - k) % nx) * 2 + core
        return remote(block(t), block(t), asem.at[1, k], arem.at[1, k], z, y, cx * 2 + 1 - core)

    def a_pair_in(k):
        t = ((cx + nx - k) % nx) * 2 + 1 - core
        return remote(block(t), block(t), asem.at[1, k], arem.at[1, k], z, y, tp)

    before = abuf.at[pl.ds(0, EDGE), :]
    after = abuf.at[pl.ds(EDGE + length, EDGE), :]
    last_own = abuf.at[pl.ds(EDGE + length - EDGE, EDGE), :]
    first_own = abuf.at[pl.ds(EDGE, EDGE), :]
    down = (sp + n * n - 1) % (n * n)
    up = (sp + 1) % (n * n)
    far = tps - 1

    def edge_next():
        return remote(last_own, before, hs.at[0, 0], hr.at[0, 0], up // n, up % n, far)

    def edge_prev():
        return remote(first_own, after, hs.at[1, 0], hr.at[1, 0], down // n, down % n, 0)

    def edge_share(side, k):
        ref = (before, after)[side]
        return remote(ref, ref, hs.at[side, k], hr.at[side, k], z, y, ((far, 0)[side] + k) % tps)

    def edge_share_in(side, k):
        ref = (before, after)[side]
        return remote(ref, ref, hs.at[side, k], hr.at[side, k], z, y, tp)

    spread1(1, 3)
    ring1(0, 1)
    spread1(3, n)
    for k in range(1, nx):
        a_out(k).start()
    a_pair(0).start()

    @pl.when((tp == far) & (sp < n * n - 1))
    def _():
        edge_next().start()

    @pl.when((tp == 0) & (sp > 0))
    def _():
        edge_prev().start()

    ring1(1, 3)
    lead2(0, 1)
    ring1(n, n + 1)
    ring1(3, 5)
    ring1(n + 1, n + 3)
    ring1(5, n)

    @pl.when((tp == far) & (sp > 0))
    def _():
        edge_share_in(0, 0).wait_recv()
        for k in range(1, tps):
            edge_share(0, k).start()

    @pl.when((tp == 0) & (sp < n * n - 1))
    def _():
        edge_share_in(1, 0).wait_recv()
        for k in range(1, tps):
            edge_share(1, k).start()

    lead2(1, 3)
    ring1(n + 3, 2 * n)
    for k in range(1, nx):
        if k != half_way(nx):
            a_in(k).wait_recv()
            a_pair(k).start()
    lead2(3, 5)
    ring1(2 * n, 3 * n)
    a_in(half_way(nx)).wait_recv()
    a_pair(half_way(nx)).start()
    lead2(5, 7)
    ring1(3 * n, 4 * n)
    lead2(7, 8)
    ring2(0, 4)

    for k in range(nx):
        a_pair_in(k).wait_recv()

    for side in range(2):
        edge_there = (sp > 0) if side == 0 else (sp < n * n - 1)
        for k in range(1, tps):

            @pl.when(edge_there & (tp == ((far, 0)[side] + k) % tps))
            def _(side=side, k=k):
                edge_share_in(side, k).wait_recv()

    steps = jnp.concatenate([step_ref[0], step_ref[1], jnp.zeros((12, dim), BF)], axis=0)
    raw = dot_nt(steps, abuf[EDGE : EDGE + length, :])[0:8]
    deltas = softplus(wide(raw.astype(BF)))
    spike = spike_ref[...]
    spikes = jnp.concatenate([spike, spike, jnp.zeros((4, length), F32)], axis=0)
    row_id = lax.broadcasted_iota(jnp.int32, (8, 1), 0)
    rates = jnp.zeros((8, 1), F32)
    for k in range(4):
        rates = jnp.where(row_id == k, rate_ref[k // 2 : k // 2 + 1, k % 2 : k % 2 + 1], rates)
    logs = spikes - deltas * rates
    logs = jnp.where(row_id < 4, logs, 0.0)
    lane = lax.broadcasted_iota(jnp.int32, (8, length), 1)
    fsum = logs
    bsum = logs
    shift = 1
    while shift < length:
        fsum = fsum + jnp.where(lane >= shift, pltpu.roll(fsum, shift, axis=1), 0.0)
        bsum = bsum + jnp.where(lane < length - shift, pltpu.roll(bsum, length - shift, axis=1), 0.0)
        shift *= 2
    run = jnp.where(row_id < 2, fsum, bsum)
    total = jnp.where(row_id < 2, fsum[:, length - 1 : length], bsum[:, 0:1])
    weight = jnp.exp(total - run) * deltas
    turned = jnp.concatenate([run, weight, jnp.exp(run), jnp.zeros((CH - 24, length), F32)], axis=0).T

    ring1(4 * n, turns)
    ring2(4, 6)

    def project1(lo, hi):
        w = w1[:, :, :, :, lo:hi].reshape(dim, hi - lo)
        if hi - lo > 128:
            got = jnp.dot(abuf[...], w, preferred_element_type=F32)
        else:
            cut = dim // 2
            got = jnp.dot(abuf[:, :cut], w[:cut], preferred_element_type=F32)
            got = got + jnp.dot(abuf[:, cut:], w[cut:], preferred_element_type=F32)
        p1[:, lo:hi] = wide(got.astype(BF))

    tb = 128 if length % 128 == 0 else rows

    def mix(lo):
        if lo == 0:
            taps = wide(xtap_ref[...])
        else:
            at = lo - 128
            taps = wide(ltap_ref[:, at // 256, at % 256 : at % 256 + 128])
        for b in range(length // tb):
            acc = None
            for k in range(5):
                term = p1[EDGE - 2 + k + b * tb : EDGE - 2 + k + (b + 1) * tb, lo : lo + 128] * taps[k : k + 1, :]
                acc = term if acc is None else acc + term
            mixed[b * tb : (b + 1) * tb, lo : lo + 128] = silu(acc).astype(BF)

    project1(0, 512)
    ring2(6, 9)
    project1(512, 640)
    ring2(9, 11)
    for j in range(5):
        mix(128 * j)
    ring2(11, 12)

    low = lax.broadcasted_iota(jnp.int32, (length, CH), 1) < HEAD
    xs_all = wide(mixed[:, 0:128])
    states = []
    for d in range(2):
        w_d = jnp.where(low, turned[:, 8 + 2 * d : 9 + 2 * d], turned[:, 9 + 2 * d : 10 + 2 * d])
        xw = (xs_all * w_d).astype(BF)
        for h in range(2):
            full = dot_tn(xw, mixed[:, 128 + 128 * h : 256 + 128 * h])
            states.append(full[HEAD * h : HEAD * h + HEAD, :])
    decay = jnp.broadcast_to(jnp.exp(total), (8, STATE))

    def packed(parts, dec):
        high = dec.astype(BF)
        rest = dec - wide(high)
        return jnp.concatenate([*parts, wide(high), rest], axis=0).astype(BF)

    for j in range(n):
        got = packed([s[sl * j : sl * j + sl, :] for s in states], decay)
        sb1[j] = got
    rb1[y] = sb1[y]

    def e1(k):
        yy = (y + k) % n
        return remote(sb1.at[yy], rb1.at[y], es.at[0, k], er.at[0, k], z, yy, tp)

    def e2(k):
        return remote(sb2, rb2.at[z], es.at[1, k], er.at[1, k], (z + k) % n, y, tp)

    def e3(k):
        yy = (y + k) % n
        return remote(sb3.at[yy], rb3.at[y], es.at[2, k], er.at[2, k], z, yy, tp)

    def e_in(which, k):
        if which == 0:
            ref = rb1.at[(y - k + n) % n]
        elif which == 1:
            ref = rb2.at[(z - k + n) % n]
        else:
            ref = rb3.at[(y - k + n) % n]
        return remote(ref, ref, es.at[which, k], er.at[which, k], z, y, tp)

    for k in range(1, n):
        e1(k).start()

    runs = [run[k : k + 1, :] for k in range(4)]
    dels = [deltas[k : k + 1, :] for k in range(4)]

    def within(h, b):
        scores = dot_nt(
            mixed[b * tb : (b + 1) * tb, 384 + 128 * h : 512 + 128 * h],
            mixed[:, 128 + 128 * h : 256 + 128 * h],
        )
        t_id = lax.broadcasted_iota(jnp.int32, (tb, length), 0) + b * tb
        s_id = lax.broadcasted_iota(jnp.int32, (tb, length), 1)
        part = turned[b * tb : (b + 1) * tb, :]
        gap_f = part[:, h : h + 1] - runs[h]
        gap_b = part[:, 2 + h : 3 + h] - runs[2 + h]
        factor = jnp.where(s_id < t_id, dels[h], jnp.where(s_id > t_id, dels[2 + h], dels[h] + dels[2 + h]))
        decays = jnp.exp(jnp.where(s_id < t_id, gap_f, jnp.where(s_id > t_id, gap_b, 0.0)))
        weights = (scores * decays * factor).astype(BF)
        keep = (lax.broadcasted_iota(jnp.int32, (length, CH), 1) // HEAD) == h
        x_h = jnp.where(keep, xs_all, 0.0).astype(BF)
        got = jnp.dot(weights, x_h, preferred_element_type=F32)
        at = slice(b * tb, (b + 1) * tb)
        yacc[at, :] = got if h == 0 else yacc[at, :] + got

    spots = [(h, b) for h in range(2) for b in range(length // tb)]
    ring2(12, 13)
    for i, (h, b) in enumerate(spots):
        within(h, b)
        ring2(13 + i, 14 + i)

    for k in range(1, n):
        e_in(0, k).wait_recv()

    def opened(ref):
        blk = wide(ref[...])
        parts = [blk[sl * q : sl * q + sl, :] for q in range(4)]
        base = 4 * sl
        decs = [blk[base + q : base + q + 1, :] + blk[base + 8 + q : base + 9 + q, :] for q in range(4)]
        return parts, decs

    carry = [jnp.zeros((sl, STATE), F32) for _ in range(4)]
    prod = [jnp.ones((1, STATE), F32) for _ in range(4)]
    for j in range(n):
        for q in range(4):
            jj = j if q < 2 else n - 1 - j
            blk = wide(rb1[jj])
            pre[jj, sl * q : sl * q + sl, :] = carry[q]
            prd[jj, q : q + 1, :] = prod[q]
            dec = blk[4 * sl + q : 4 * sl + q + 1, :] + blk[4 * sl + 8 + q : 4 * sl + 9 + q, :]
            carry[q] = carry[q] * dec + blk[sl * q : sl * q + sl, :]
            prod[q] = prod[q] * dec
    prods = jnp.concatenate([*prod, jnp.zeros((4, STATE), F32)], axis=0)
    sb2[...] = packed(carry, prods)
    for k in range(1, n):
        e2(k).start()
    ring2(19, 24)
    for k in range(1, n):
        e_in(1, k).wait_recv()
    entry = [jnp.zeros((sl, STATE), F32) for _ in range(4)]
    for j in range(n):
        for q in range(4):
            jj = j if q < 2 else n - 1 - j
            blk = wide(rb2[jj])
            dec = blk[4 * sl + q : 4 * sl + q + 1, :] + blk[4 * sl + 8 + q : 4 * sl + 9 + q, :]
            ahead = (jj < z) if q < 2 else (jj > z)
            entry[q] = jnp.where(ahead, entry[q] * dec + blk[sl * q : sl * q + sl, :], entry[q])
    for j in range(n):
        parts = [entry[q] * prd[j, q : q + 1, :] + pre[j, sl * q : sl * q + sl, :] for q in range(4)]
        sb3[j] = jnp.concatenate(parts, axis=0).astype(BF)
    rb3[y] = sb3[y]
    for k in range(1, n):
        e3(k).start()

    ring2(24, turns)

    def project2(lo, hi):
        got = jnp.dot(abuf[...], w2[:, :, :, :, lo:hi].reshape(dim, hi - lo), preferred_element_type=F32)
        p2[:, lo:hi] = wide(got.astype(BF))

    project2(0, 256)
    project2(256, 512)
    p2[:, 128:256] = wide((p2[:, 128:256] * p2[:, 256:384]).astype(BF))
    ctaps = wide(ctap_ref[...])
    for b in range(length // tb):
        acc = None
        for k in range(3):
            term = p2[EDGE - 1 + k + b * tb : EDGE - 1 + k + (b + 1) * tb, 128:256] * ctaps[k : k + 1, :]
            acc = term if acc is None else acc + term
        ycat[b * tb : (b + 1) * tb, 0:128] = (p2[EDGE + b * tb : EDGE + (b + 1) * tb, 0:128] * acc).astype(BF)

    for k in range(1, n):
        e_in(2, k).wait_recv()
    blocks = [wide(rb3[j]) for j in range(n)]
    arrived = [
        jnp.concatenate([blk[sl * q : sl * q + sl, :] for blk in blocks], axis=0).astype(BF) for q in range(4)
    ]
    none = jnp.zeros((HEAD, STATE), BF)
    y_all = yacc[...]
    for d in range(2):
        top = jnp.concatenate([arrived[2 * d], none], axis=1)
        bottom = jnp.concatenate([none, arrived[2 * d + 1]], axis=1)
        into = dot_nt(mixed[:, 384:640], jnp.concatenate([top, bottom], axis=0))
        grow = jnp.where(low, turned[:, 16 + 2 * d : 17 + 2 * d], turned[:, 17 + 2 * d : 18 + 2 * d])
        y_all = y_all + into * grow
    g = y_all * silu(p2[EDGE : EDGE + length, 384:512])
    sq = g * g
    mean0 = jnp.sum(jnp.where(low, sq, 0.0), axis=-1, keepdims=True) / HEAD
    mean1 = jnp.sum(jnp.where(low, 0.0, sq), axis=-1, keepdims=True) / HEAD
    inv = jnp.where(low, lax.rsqrt(mean0 + EPS), lax.rsqrt(mean1 + EPS))
    ycat[:, 128:256] = (g * inv * wide(lane_ref[...])).astype(BF)

    def to_pair(c):
        cols = slice(c * wcol, (c + 1) * wcol)
        return remote(
            obf.at[:, 1 - core, :, cols], prx.at[:, :, cols], os_.at[c], or_.at[c], z, y, cx * 2 + 1 - core
        )

    def to_owner(c, k):
        cols = slice(c * wcol, (c + 1) * wcol)
        xx = (cx + k) % nx
        return remote(
            xsend.at[xx, :, cols], xrecv.at[k, :, cols], xs.at[c, k], xr.at[c, k], z, y, xx * 2 + core
        )

    exits = w2[:, :, :, :, 512:768].reshape(dim, 2 * CH)
    for c in range(ncol):
        cols = slice(c * wcol, (c + 1) * wcol)
        got = dot_nt(ycat[...], exits[c * wcol : (c + 1) * wcol, :])
        obf[:, :, :, cols] = got.astype(BF).reshape(nx, 2, rows, wcol)
        to_pair(c).start()
    for c in range(ncol):
        cols = slice(c * wcol, (c + 1) * wcol)
        to_pair(c).wait_recv()
        for xx in range(nx):
            both = wide(obf[xx, core, :, cols]) + wide(prx[xx, :, cols])
            xsend[xx, :, cols] = both.astype(BF)
        for k in range(1, nx):
            to_owner(c, k).start()
    drain1()
    drain2()
    for c in range(ncol):
        cols = slice(c * wcol, (c + 1) * wcol)
        both = wide(obf[cx, core, :, cols]) + wide(prx[cx, :, cols])
        for k in range(1, nx):
            to_owner(c, k).wait_recv()
            both = both + wide(xrecv[k, :, cols])
        out_ref[:, cols] = both.astype(BF)

    for c in range(ncol):
        to_pair(c).wait_send()
        for k in range(1, nx):
            to_owner(c, k).wait_send()
    for k in range(1, n):
        e1(k).wait_send()
        e2(k).wait_send()
        e3(k).wait_send()
    for k in range(1, nx):
        a_out(k).wait_send()
    for k in range(nx):
        a_pair(k).wait_send()

    @pl.when((tp == far) & (sp < n * n - 1))
    def _():
        edge_next().wait_send()

    @pl.when((tp == 0) & (sp > 0))
    def _():
        edge_prev().wait_send()

    @pl.when((tp == far) & (sp > 0))
    def _():
        for k in range(1, tps):
            edge_share(0, k).wait_send()

    @pl.when((tp == 0) & (sp < n * n - 1))
    def _():
        for k in range(1, tps):
            edge_share(1, k).wait_send()


def half_way(nx):
    return nx // 2


def run_layer(n, tps, ncol, *args):
    (
        x,
        gain,
        slide,
        rec,
        lat,
        step,
        ctap,
        xtap,
        ltap,
        rate,
        spike,
        lane,
        cexit,
        sexit,
    ) = args
    rows, dim = x.shape
    length = rows * tps
    tall = length + 2 * EDGE
    nx = tps // 2
    half = n // 2
    sl = HEAD // n
    vm = pltpu.VMEM
    dma = pltpu.SemaphoreType.DMA
    vmem = pl.BlockSpec(memory_space=pltpu.VMEM)
    specs = [pl.BlockSpec(memory_space=pltpu.HBM)] * 14
    operands = (
        x,
        gain.reshape(dim // 128, 128),
        slide,
        rec,
        lat,
        step.transpose(1, 2, 0),
        ctap,
        xtap,
        ltap,
        rate,
        spike.T,
        lane.reshape(1, CH),
        cexit.T,
        sexit.T,
    )
    return pl.pallas_call(
        functools.partial(layer, n, tps),
        out_shape=jax.ShapeDtypeStruct((rows, dim), BF),
        in_specs=specs,
        out_specs=vmem,
        scratch_shapes=[
            vm((tall, dim), BF),
            vm((n, n, 2, 16, 640), BF),
            vm((n, n, 2, 16, 768), BF),
            vm((tall, 640), F32),
            vm((tall, 512), F32),
            vm((length, 640), BF),
            vm((length, 256), BF),
            vm((length, 128), F32),
            vm((n, 4 * sl + 16, STATE), BF),
            vm((n, 4 * sl + 16, STATE), BF),
            vm((4 * sl + 16, STATE), BF),
            vm((n, 4 * sl + 16, STATE), BF),
            vm((n, 4 * sl, STATE), BF),
            vm((n, 4 * sl, STATE), BF),
            vm((n, 4 * sl, STATE), F32),
            vm((n, 8, STATE), F32),
            vm((nx, 2, rows, dim), BF),
            vm((nx, rows, dim), BF),
            vm((nx, rows, dim), BF),
            vm((nx, rows, dim), BF),
            dma((2, 2, half + 1, n)),
            dma((2, 2, half + 1, n)),
            dma((2, 2, half + 1, n)),
            dma((2, 2, half + 1, n)),
            dma((2, 2, n)),
            dma((2, 2, n)),
            dma((2, nx)),
            dma((2, nx)),
            dma((2, tps)),
            dma((2, tps)),
            dma((3, n)),
            dma((3, n)),
            dma((ncol,)),
            dma((ncol,)),
            dma((ncol, nx)),
            dma((ncol, nx)),
            *[vm(v.shape, v.dtype) for v in operands],
            dma((14,)),
        ],
        compiler_params=pltpu.CompilerParams(
            collective_id=0, has_side_effects=True, vmem_limit_bytes=60 * 1024 * 1024
        ),
        name="layer",
    )(*operands)


def solution(mesh):
    n = 8 if mesh.shape["sp"] == 64 else int(round(mesh.shape["sp"] ** 0.5))
    sp_tp = ("sp", "tp")
    return jax.shard_map(
        functools.partial(run_layer, n, mesh.shape["tp"], 4),
        mesh=mesh,
        in_specs=(
            P(sp_tp, None),
            P(),
            P(None, "sp", "tp"),
            P(None, "sp", "tp"),
            P(None, "sp", "tp"),
            P(None, None, "tp"),
            P(None, "tp"),
            P(None, "tp"),
            P(None, None, "tp"),
            P(None, "tp"),
            P("sp", "tp"),
            P("tp"),
            P("tp", "sp"),
            P("tp", "sp"),
        ),
        out_specs=P(sp_tp, None),
        check_vma=False,
    )
```

```python
import functools

import jax
import jax.numpy as jnp
from jax import lax
from jax.experimental import pallas as pl
from jax.experimental.pallas import tpu as pltpu
from jax.sharding import PartitionSpec as P

HEAD = 64
STATE = 128
CH = 128
EDGE = 16
EPS = 1e-05
BF = jnp.bfloat16
F32 = jnp.float32
MESH_IDS = pl.DeviceIdType.MESH


def wide(v):
    return v.astype(F32)


def dot_nt(a, b):
    return lax.dot_general(a, b, (((1,), (1,)), ((), ())), preferred_element_type=F32)


def dot_tn(a, b):
    return lax.dot_general(a, b, (((0,), (0,)), ((), ())), preferred_element_type=F32)


def silu(v):
    return v * jax.nn.sigmoid(v)


def softplus(v):
    return jnp.maximum(v, 0.0) + jnp.log1p(jnp.exp(-jnp.abs(v)))


def layer(
    n,
    tps,
    x_hbm,
    gain_hbm,
    slide_hbm,
    rec_hbm,
    lat_hbm,
    step_hbm,
    ctap_hbm,
    xtap_hbm,
    ltap_hbm,
    rate_hbm,
    spike_hbm,
    lane_hbm,
    cexit_hbm,
    sexit_hbm,
    out_ref,
    abuf,
    w1,
    w2,
    p1,
    p2,
    mixed,
    ycat,
    yacc,
    sb1,
    rb1,
    sb2,
    rb2,
    sb3,
    rb3,
    pre,
    prd,
    obf,
    prx,
    xsend,
    xrecv,
    lrecv,
    s1,
    r1,
    s2,
    r2,
    ps,
    pr,
    asem,
    arem,
    hs,
    hr,
    es,
    er,
    os_,
    or_,
    xs,
    xr,
    x_ref,
    gain_ref,
    slide_ref,
    rec_ref,
    lat_ref,
    step_ref,
    ctap_ref,
    xtap_ref,
    ltap_ref,
    rate_ref,
    spike_ref,
    lane_ref,
    cexit_ref,
    sexit_ref,
    ins,
):
    rows = x_ref.shape[0]
    dim = x_ref.shape[1]
    nx = tps // 2
    length = rows * tps
    half = n // 2
    sl = HEAD // n
    ncol = or_.shape[0]
    wcol = dim // ncol
    sp = lax.axis_index("sp")
    tp = lax.axis_index("tp")
    z = sp // n
    y = sp % n
    cx = tp // 2
    core = tp % 2

    def remote(src, dst, ss, rs, zz, yy, tt):
        return pltpu.make_async_remote_copy(
            src_ref=src,
            dst_ref=dst,
            send_sem=ss,
            recv_sem=rs,
            device_id=(zz * n + yy, tt),
            device_id_type=MESH_IDS,
        )

    given = (
        (x_hbm, x_ref),
        (gain_hbm, gain_ref),
        (slide_hbm, slide_ref),
        (rec_hbm, rec_ref),
        (lat_hbm, lat_ref),
        (step_hbm, step_ref),
        (ctap_hbm, ctap_ref),
        (xtap_hbm, xtap_ref),
        (ltap_hbm, ltap_ref),
        (rate_hbm, rate_ref),
        (spike_hbm, spike_ref),
        (lane_hbm, lane_ref),
        (cexit_hbm, cexit_ref),
        (sexit_hbm, sexit_ref),
    )
    loads = [pltpu.make_async_copy(src, dst, ins.at[i]) for i, (src, dst) in enumerate(given)]
    for load in loads:
        load.start()

    bar = pltpu.get_barrier_semaphore()

    def greet(s, t):
        pl.semaphore_signal(bar, inc=1, device_id=(s, t), device_id_type=MESH_IDS)

    for k in range(1, n):
        greet(z * n + (y + k) % n, tp)
        greet(((z + k) % n) * n + y, tp)
    for k in range(1, tps):
        greet(sp, (tp + k) % tps)
    greet((sp + 1) % (n * n), tp)
    greet((sp + n * n - 1) % (n * n), tp)

    for load in loads:
        load.wait()
    xf = wide(x_ref[...])
    scale = lax.rsqrt(jnp.mean(xf * xf, axis=-1, keepdims=True) + EPS)
    own_rows = pl.ds(pl.multiple_of(EDGE + rows * tp, 16), rows)
    gains = wide(gain_ref[...])
    for j in range(dim // 128):
        cols = slice(128 * j, 128 * j + 128)
        abuf[own_rows, cols] = (xf[:, cols] * scale * gains[j : j + 1, :]).astype(BF)

    @pl.when(sp == 0)
    def _():
        abuf[pl.ds(0, EDGE), :] = jnp.zeros((EDGE, dim), BF)

    @pl.when(sp == n * n - 1)
    def _():
        abuf[pl.ds(EDGE + length, EDGE), :] = jnp.zeros((EDGE, dim), BF)

    for h in range(2):
        cut = slice(16 * h, 16 * h + 16)
        w1[z, y, h, :, 0:128] = rec_ref[1, cut, :]
        w1[z, y, h, :, 128:384] = lat_ref[0, cut, :]
        w1[z, y, h, :, 384:640] = lat_ref[1, cut, :]
        w2[z, y, h, :, 0:128] = slide_ref[0, cut, :]
        w2[z, y, h, :, 128:256] = slide_ref[1, cut, :]
        w2[z, y, h, :, 256:384] = slide_ref[2, cut, :]
        w2[z, y, h, :, 384:512] = rec_ref[0, cut, :]
        w2[z, y, h, :, 512:640] = cexit_ref[cut, :]
        w2[z, y, h, :, 640:768] = sexit_ref[cut, :]

    pl.semaphore_wait(bar, 2 * (n - 1) + (tps - 1) + 2)

    def moved(h, phase, k):
        on_y = (h == 0) == (phase == 1)
        return (z, (y + k + n) % n) if on_y else ((z + k + n) % n, y)

    def piece(h, c, s, d):
        off = -((c + 1) // 2) if c % 2 else c // 2
        return place(h, off, s, d)

    def place(h, off, s, d):
        if h == 0:
            return (z - d * s + n) % n, (y + off + n) % n, 0
        return (z + off + n) % n, (y - d * s + n) % n, 1

    def ring_one(w, ss, rs, qs, qr, rnd, straight):
        def first(h, c, nxt):
            d = 1 if nxt % 2 else -1
            ref = w.at[piece(h, c, 0, 1)]
            zz, yy = moved(h, 1, d)
            return remote(ref, ref, qs.at[rnd], qr.at[rnd, nxt], zz, yy, tp)

        def first_in(c):
            ref = w.at[0, 0]
            remote(ref, ref, qs.at[rnd], qr.at[rnd, c], z, y, tp).wait_recv()

        def second(h, off, c, s, di, d):
            ref = w.at[place(h, off, s, d)]
            zz, yy = moved(h, 2, d)
            return remote(ref, ref, ss.at[0], rs.at[s, c], zz, yy, tp)

        def second_in(c, s):
            ref = w.at[0, 0:2] if s < half else w.at[0, 0]
            remote(ref, ref, ss.at[0], rs.at[s - 1, c], z, y, tp).wait_recv()

        def offset(c):
            return jnp.where(c % 2 == 1, -((c + 1) // 2), c // 2)

        def direct(h, c):
            d = (c + 1) // 2 if c % 2 else -(c // 2)
            ref = w.at[piece(h, 0, 0, 1)]
            zz, yy = moved(h, 1, d)
            return remote(ref, ref, qs.at[rnd], qr.at[rnd, c], zz, yy, tp)

        def spread(lo, hi):
            for c in range(lo, hi):
                for h in range(2):
                    direct(h, c).start()

        def lead(lo, hi):
            for c in range(lo, hi):
                if c > 0:
                    first_in(c)
                for h in range(2):
                    if c == 0:
                        first(h, 0, 1).start()
                        first(h, 0, 2).start()
                    elif c + 2 < n:
                        first(h, c, c + 2).start()

        def start(c):
            if straight and c > 0:
                first_in(c)
            for h in range(2):
                off = -((c + 1) // 2) if c % 2 else c // 2
                for di, d in ((0, 1), (1, -1)):
                    if half > 1 or di == c % 2:
                        second(h, off, c, 0, di, d).start()

        def pass_on(s, c):
            off = offset(c)
            second_in(c, s)
            for h in range(2):
                if s < half - 1:
                    for di, d in ((0, 1), (1, -1)):
                        second(h, off, c, s, di, d).start()
                else:
                    di = c % 2
                    second(h, off, c, s, di, 1 - 2 * di).start()

        def advance(lo, hi):
            while lo < hi:
                s, c = divmod(lo, n)
                if s == 0:
                    start(c)
                    lo += 1
                elif s < half:
                    stop = min(hi, (s + 1) * n)

                    @pl.loop(c, c + stop - lo)
                    def _(cc, s=s):
                        pass_on(s, cc)

                    lo = stop
                else:
                    stop = min(hi, (s + 1) * n)

                    @pl.loop(c, c + stop - lo)
                    def _(cc, s=s):
                        second_in(cc, s)

                    lo = stop

        def drain():
            lead_all = w.at[0, 0 : n - 1]
            remote(lead_all, lead_all, qs.at[rnd], qr.at[rnd, 0], z, y, tp).wait_send()
            ring_all = w.at[0 : n - 1]
            remote(ring_all, ring_all, ss.at[0], rs.at[0, 0], z, y, tp).wait_send()

        return advance, drain, spread, lead

    turns = (half + 1) * n
    ring1, drain1, spread1, _ = ring_one(w1, s1, r1, ps, pr, 0, True)
    ring2, drain2, _, lead2 = ring_one(w2, s2, r2, ps, pr, 1, False)

    def block(t):
        return abuf.at[pl.ds(pl.multiple_of(EDGE + rows * t, 16), rows), :]

    def a_out(k):
        return remote(block(tp), block(tp), asem.at[0], arem.at[k], z, y, ((cx + k) % nx) * 2 + core)

    def a_in(k):
        t = ((cx + nx - k) % nx) * 2 + core
        return remote(block(t), block(t), asem.at[0], arem.at[k], z, y, tp)

    def a_pair(k):
        t = ((cx + nx - k) % nx) * 2 + core
        return remote(block(t), block(t), asem.at[1], arem.at[nx], z, y, cx * 2 + 1 - core)

    def a_wait(blocks, which):
        ref = abuf.at[pl.ds(0, rows * blocks), :]
        return remote(ref, ref, asem.at[which], arem.at[nx], z, y, tp)

    before = abuf.at[pl.ds(0, EDGE), :]
    after = abuf.at[pl.ds(EDGE + length, EDGE), :]
    last_own = abuf.at[pl.ds(EDGE + length - EDGE, EDGE), :]
    first_own = abuf.at[pl.ds(EDGE, EDGE), :]
    down = (sp + n * n - 1) % (n * n)
    up = (sp + 1) % (n * n)
    far = tps - 1

    def edge_next():
        return remote(last_own, before, hs.at[0, 0], hr.at[0], up // n, up % n, far)

    def edge_prev():
        return remote(first_own, after, hs.at[1, 0], hr.at[1], down // n, down % n, 0)

    def edge_share(side, k):
        ref = (before, after)[side]
        return remote(ref, ref, hs.at[side, 1], hr.at[side], z, y, ((far, 0)[side] + k) % tps)

    def edge_in(side):
        ref = (before, after)[side]
        remote(ref, ref, hs.at[side, 1], hr.at[side], z, y, tp).wait_recv()

    def edge_sent(side):
        ref = abuf.at[pl.ds(0, EDGE * (tps - 1)), :]
        remote(ref, ref, hs.at[side, 1], hr.at[side], z, y, tp).wait_send()

    spread1(1, 3)
    ring1(0, 1)
    spread1(3, n)
    for k in range(1, nx):
        a_out(k).start()
    a_pair(0).start()

    @pl.when((tp == far) & (sp < n * n - 1))
    def _():
        edge_next().start()

    @pl.when((tp == 0) & (sp > 0))
    def _():
        edge_prev().start()

    ring1(1, 3)
    lead2(0, 1)
    ring1(n, n + 1)
    ring1(3, 5)
    ring1(n + 1, n + 3)
    ring1(5, n)

    @pl.when((tp == far) & (sp > 0))
    def _():
        edge_in(0)
        for k in range(1, tps):
            edge_share(0, k).start()

    @pl.when((tp == 0) & (sp < n * n - 1))
    def _():
        edge_in(1)
        for k in range(1, tps):
            edge_share(1, k).start()

    lead2(1, 3)
    ring1(n + 3, 2 * n)
    for k in range(1, nx):
        if k != half_way(nx):
            a_in(k).wait_recv()
            a_pair(k).start()
    lead2(3, 5)
    ring1(2 * n, 3 * n)
    a_in(half_way(nx)).wait_recv()
    a_pair(half_way(nx)).start()
    lead2(5, 7)
    ring1(3 * n, 4 * n)
    lead2(7, 8)
    ring2(0, 4)

    a_wait(nx, 1).wait_recv()

    @pl.when((tp != far) & (sp > 0))
    def _():
        edge_in(0)

    @pl.when((tp != 0) & (sp < n * n - 1))
    def _():
        edge_in(1)

    steps = jnp.concatenate([step_ref[0], step_ref[1], jnp.zeros((12, dim), BF)], axis=0)
    raw = dot_nt(steps, abuf[EDGE : EDGE + length, :])[0:8]
    deltas = softplus(wide(raw.astype(BF)))
    spike = spike_ref[...]
    spikes = jnp.concatenate([spike, spike, jnp.zeros((4, length), F32)], axis=0)
    row_id = lax.broadcasted_iota(jnp.int32, (8, 1), 0)
    rates = jnp.zeros((8, 1), F32)
    for k in range(4):
        rates = jnp.where(row_id == k, rate_ref[k // 2 : k // 2 + 1, k % 2 : k % 2 + 1], rates)
    logs = spikes - deltas * rates
    logs = jnp.where(row_id < 4, logs, 0.0)
    lane = lax.broadcasted_iota(jnp.int32, (8, length), 1)
    fsum = logs
    bsum = logs
    shift = 1
    while shift < length:
        fsum = fsum + jnp.where(lane >= shift, pltpu.roll(fsum, shift, axis=1), 0.0)
        bsum = bsum + jnp.where(lane < length - shift, pltpu.roll(bsum, length - shift, axis=1), 0.0)
        shift *= 2
    run = jnp.where(row_id < 2, fsum, bsum)
    total = jnp.where(row_id < 2, fsum[:, length - 1 : length], bsum[:, 0:1])
    weight = jnp.exp(total - run) * deltas
    turned = jnp.concatenate([run, weight, jnp.exp(run), jnp.zeros((CH - 24, length), F32)], axis=0).T

    ring1(4 * n, turns)
    ring2(4, 6)

    def project1(lo, hi):
        w = w1[:, :, :, :, lo:hi].reshape(dim, hi - lo)
        if hi - lo > 128:
            got = jnp.dot(abuf[...], w, preferred_element_type=F32)
        else:
            cut = dim // 2
            got = jnp.dot(abuf[:, :cut], w[:cut], preferred_element_type=F32)
            got = got + jnp.dot(abuf[:, cut:], w[cut:], preferred_element_type=F32)
        p1[:, lo:hi] = wide(got.astype(BF))

    tb = 128 if length % 128 == 0 else rows

    def mix(lo):
        if lo == 0:
            taps = wide(xtap_ref[...])
        else:
            at = lo - 128
            taps = wide(ltap_ref[:, at // 256, at % 256 : at % 256 + 128])
        for b in range(length // tb):
            acc = None
            for k in range(5):
                term = p1[EDGE - 2 + k + b * tb : EDGE - 2 + k + (b + 1) * tb, lo : lo + 128] * taps[k : k + 1, :]
                acc = term if acc is None else acc + term
            mixed[b * tb : (b + 1) * tb, lo : lo + 128] = silu(acc).astype(BF)

    project1(0, 512)
    ring2(6, 9)
    project1(512, 640)
    ring2(9, 11)
    for j in range(5):
        mix(128 * j)
    ring2(11, 12)

    low = lax.broadcasted_iota(jnp.int32, (length, CH), 1) < HEAD
    xs_all = wide(mixed[:, 0:128])
    states = []
    for d in range(2):
        w_d = jnp.where(low, turned[:, 8 + 2 * d : 9 + 2 * d], turned[:, 9 + 2 * d : 10 + 2 * d])
        xw = (xs_all * w_d).astype(BF)
        for h in range(2):
            full = dot_tn(xw, mixed[:, 128 + 128 * h : 256 + 128 * h])
            states.append(full[HEAD * h : HEAD * h + HEAD, :])
    decay = jnp.broadcast_to(jnp.exp(total), (8, STATE))

    def packed(parts, dec):
        high = dec.astype(BF)
        rest = dec - wide(high)
        return jnp.concatenate([*parts, wide(high), rest], axis=0).astype(BF)

    for j in range(n):
        got = packed([s[sl * j : sl * j + sl, :] for s in states], decay)
        sb1[j] = got
    rb1[y] = sb1[y]

    def e1(k):
        yy = (y + k) % n
        return remote(sb1.at[yy], rb1.at[y], es.at[0], er.at[0], z, yy, tp)

    def e2(k):
        return remote(sb2, rb2.at[z], es.at[1], er.at[1], (z + k) % n, y, tp)

    def e3(k):
        yy = (y + k) % n
        return remote(sb3.at[yy], rb3.at[y], es.at[2], er.at[2], z, yy, tp)

    def e_all(which):
        ref = (rb1, rb2, rb3)[which].at[0 : n - 1]
        return remote(ref, ref, es.at[which], er.at[which], z, y, tp)

    for k in range(1, n):
        e1(k).start()

    runs = [run[k : k + 1, :] for k in range(4)]
    dels = [deltas[k : k + 1, :] for k in range(4)]

    def within(h, b):
        scores = dot_nt(
            mixed[b * tb : (b + 1) * tb, 384 + 128 * h : 512 + 128 * h],
            mixed[:, 128 + 128 * h : 256 + 128 * h],
        )
        t_id = lax.broadcasted_iota(jnp.int32, (tb, length), 0) + b * tb
        s_id = lax.broadcasted_iota(jnp.int32, (tb, length), 1)
        part = turned[b * tb : (b + 1) * tb, :]
        gap_f = part[:, h : h + 1] - runs[h]
        gap_b = part[:, 2 + h : 3 + h] - runs[2 + h]
        factor = jnp.where(s_id < t_id, dels[h], jnp.where(s_id > t_id, dels[2 + h], dels[h] + dels[2 + h]))
        decays = jnp.exp(jnp.where(s_id < t_id, gap_f, jnp.where(s_id > t_id, gap_b, 0.0)))
        weights = (scores * decays * factor).astype(BF)
        keep = (lax.broadcasted_iota(jnp.int32, (length, CH), 1) // HEAD) == h
        x_h = jnp.where(keep, xs_all, 0.0).astype(BF)
        got = jnp.dot(weights, x_h, preferred_element_type=F32)
        at = slice(b * tb, (b + 1) * tb)
        yacc[at, :] = got if h == 0 else yacc[at, :] + got

    spots = [(h, b) for h in range(2) for b in range(length // tb)]
    ring2(12, 13)
    for i, (h, b) in enumerate(spots):
        within(h, b)
        ring2(13 + i, 14 + i)

    e_all(0).wait_recv()

    def opened(ref):
        blk = wide(ref[...])
        parts = [blk[sl * q : sl * q + sl, :] for q in range(4)]
        base = 4 * sl
        decs = [blk[base + q : base + q + 1, :] + blk[base + 8 + q : base + 9 + q, :] for q in range(4)]
        return parts, decs

    carry = [jnp.zeros((sl, STATE), F32) for _ in range(4)]
    prod = [jnp.ones((1, STATE), F32) for _ in range(4)]
    for j in range(n):
        for q in range(4):
            jj = j if q < 2 else n - 1 - j
            blk = wide(rb1[jj])
            pre[jj, sl * q : sl * q + sl, :] = carry[q]
            prd[jj, q : q + 1, :] = prod[q]
            dec = blk[4 * sl + q : 4 * sl + q + 1, :] + blk[4 * sl + 8 + q : 4 * sl + 9 + q, :]
            carry[q] = carry[q] * dec + blk[sl * q : sl * q + sl, :]
            prod[q] = prod[q] * dec
    prods = jnp.concatenate([*prod, jnp.zeros((4, STATE), F32)], axis=0)
    sb2[...] = packed(carry, prods)
    for k in range(1, n):
        e2(k).start()
    ring2(19, 24)
    e_all(1).wait_recv()
    entry = [jnp.zeros((sl, STATE), F32) for _ in range(4)]
    for j in range(n):
        for q in range(4):
            jj = j if q < 2 else n - 1 - j
            blk = wide(rb2[jj])
            dec = blk[4 * sl + q : 4 * sl + q + 1, :] + blk[4 * sl + 8 + q : 4 * sl + 9 + q, :]
            ahead = (jj < z) if q < 2 else (jj > z)
            entry[q] = jnp.where(ahead, entry[q] * dec + blk[sl * q : sl * q + sl, :], entry[q])
    for j in range(n):
        parts = [entry[q] * prd[j, q : q + 1, :] + pre[j, sl * q : sl * q + sl, :] for q in range(4)]
        sb3[j] = jnp.concatenate(parts, axis=0).astype(BF)
    rb3[y] = sb3[y]
    for k in range(1, n):
        e3(k).start()

    ring2(24, turns)

    def project2(lo, hi):
        got = jnp.dot(abuf[...], w2[:, :, :, :, lo:hi].reshape(dim, hi - lo), preferred_element_type=F32)
        p2[:, lo:hi] = wide(got.astype(BF))

    project2(0, 256)
    project2(256, 512)
    p2[:, 128:256] = wide((p2[:, 128:256] * p2[:, 256:384]).astype(BF))
    ctaps = wide(ctap_ref[...])
    for b in range(length // tb):
        acc = None
        for k in range(3):
            term = p2[EDGE - 1 + k + b * tb : EDGE - 1 + k + (b + 1) * tb, 128:256] * ctaps[k : k + 1, :]
            acc = term if acc is None else acc + term
        ycat[b * tb : (b + 1) * tb, 0:128] = (p2[EDGE + b * tb : EDGE + (b + 1) * tb, 0:128] * acc).astype(BF)

    e_all(2).wait_recv()
    blocks = [wide(rb3[j]) for j in range(n)]
    arrived = [
        jnp.concatenate([blk[sl * q : sl * q + sl, :] for blk in blocks], axis=0).astype(BF) for q in range(4)
    ]
    none = jnp.zeros((HEAD, STATE), BF)
    y_all = yacc[...]
    for d in range(2):
        top = jnp.concatenate([arrived[2 * d], none], axis=1)
        bottom = jnp.concatenate([none, arrived[2 * d + 1]], axis=1)
        into = dot_nt(mixed[:, 384:640], jnp.concatenate([top, bottom], axis=0))
        grow = jnp.where(low, turned[:, 16 + 2 * d : 17 + 2 * d], turned[:, 17 + 2 * d : 18 + 2 * d])
        y_all = y_all + into * grow
    g = y_all * silu(p2[EDGE : EDGE + length, 384:512])
    sq = g * g
    mean0 = jnp.sum(jnp.where(low, sq, 0.0), axis=-1, keepdims=True) / HEAD
    mean1 = jnp.sum(jnp.where(low, 0.0, sq), axis=-1, keepdims=True) / HEAD
    inv = jnp.where(low, lax.rsqrt(mean0 + EPS), lax.rsqrt(mean1 + EPS))
    ycat[:, 128:256] = (g * inv * wide(lane_ref[...])).astype(BF)

    def span(c):
        return slice(c * wcol, (c + 1) * wcol)

    def to_pair(c):
        return remote(
            obf.at[:, 1 - core, :, span(c)], prx.at[:, :, span(c)], os_.at[0], or_.at[c], z, y, cx * 2 + 1 - core
        )

    right = (cx + 1) % nx
    left = (cx + nx - 1) % nx
    opposite = (cx + 2) % nx

    def relay(c):
        xx = right if c < ncol // 2 else left
        return remote(
            xsend.at[opposite, :, span(c)], lrecv.at[:, span(c)], xs.at[0], xr.at[0, c], z, y, xx * 2 + core
        )

    def to_owner(c, side):
        xx = (right, left)[side]
        return remote(
            xsend.at[xx, :, span(c)], xrecv.at[side, :, span(c)], xs.at[1], xr.at[1, c], z, y, xx * 2 + core
        )

    def owner_in(c):
        ref = xrecv.at[:, :, span(c)]
        remote(ref, ref, xs.at[1], xr.at[1, c], z, y, tp).wait_recv()

    def chip_sum(xx, c):
        return wide(obf[xx, core, :, span(c)]) + wide(prx[xx, :, span(c)])

    order = [c for pair in zip(range(ncol // 2), range(ncol // 2, ncol)) for c in pair]
    exits = w2[:, :, :, :, 512:768].reshape(dim, 2 * CH)
    for c in order:
        got = dot_nt(ycat[...], exits[c * wcol : (c + 1) * wcol, :])
        obf[:, :, :, span(c)] = got.astype(BF).reshape(nx, 2, rows, wcol)
        to_pair(c).start()
    for c in order:
        to_pair(c).wait_recv()
        xsend[opposite, :, span(c)] = chip_sum(opposite, c).astype(BF)
        relay(c).start()
        side = 1 if c < ncol // 2 else 0
        xx = (right, left)[side]
        xsend[xx, :, span(c)] = chip_sum(xx, c).astype(BF)
        to_owner(c, side).start()
    for c in order:
        relay(c).wait_recv()
        side = 0 if c < ncol // 2 else 1
        xx = (right, left)[side]
        xsend[xx, :, span(c)] = (chip_sum(xx, c) + wide(lrecv[:, span(c)])).astype(BF)
        to_owner(c, side).start()
    drain1()
    drain2()
    for c in order:
        own = chip_sum(cx, c)
        owner_in(c)
        out_ref[:, span(c)] = (own + wide(xrecv[0, :, span(c)]) + wide(xrecv[1, :, span(c)])).astype(BF)

    remote(prx, prx, os_.at[0], or_.at[0], z, y, tp).wait_send()
    relayed = xsend.at[0]
    remote(relayed, relayed, xs.at[0], xr.at[0, 0], z, y, tp).wait_send()
    owned = xsend.at[0:2]
    remote(owned, owned, xs.at[1], xr.at[1, 0], z, y, tp).wait_send()
    for which in range(3):
        e_all(which).wait_send()
    a_wait(nx - 1, 0).wait_send()
    a_wait(nx, 1).wait_send()

    @pl.when((tp == far) & (sp < n * n - 1))
    def _():
        edge_next().wait_send()

    @pl.when((tp == 0) & (sp > 0))
    def _():
        edge_prev().wait_send()

    @pl.when((tp == far) & (sp > 0))
    def _():
        edge_sent(0)

    @pl.when((tp == 0) & (sp < n * n - 1))
    def _():
        edge_sent(1)


def half_way(nx):
    return nx // 2


def run_layer(n, tps, ncol, *args):
    (
        x,
        gain,
        slide,
        rec,
        lat,
        step,
        ctap,
        xtap,
        ltap,
        rate,
        spike,
        lane,
        cexit,
        sexit,
    ) = args
    rows, dim = x.shape
    length = rows * tps
    tall = length + 2 * EDGE
    nx = tps // 2
    half = n // 2
    sl = HEAD // n
    vm = pltpu.VMEM
    dma = pltpu.SemaphoreType.DMA
    vmem = pl.BlockSpec(memory_space=pltpu.VMEM)
    specs = [pl.BlockSpec(memory_space=pltpu.HBM)] * 14
    operands = (
        x,
        gain.reshape(dim // 128, 128),
        slide,
        rec,
        lat,
        step.transpose(1, 2, 0),
        ctap,
        xtap,
        ltap,
        rate,
        spike.T,
        lane.reshape(1, CH),
        cexit.T,
        sexit.T,
    )
    return pl.pallas_call(
        functools.partial(layer, n, tps),
        out_shape=jax.ShapeDtypeStruct((rows, dim), BF),
        in_specs=specs,
        out_specs=vmem,
        scratch_shapes=[
            vm((tall, dim), BF),
            vm((n, n, 2, 16, 640), BF),
            vm((n, n, 2, 16, 768), BF),
            vm((tall, 640), F32),
            vm((tall, 512), F32),
            vm((length, 640), BF),
            vm((length, 256), BF),
            vm((length, 128), F32),
            vm((n, 4 * sl + 16, STATE), BF),
            vm((n, 4 * sl + 16, STATE), BF),
            vm((4 * sl + 16, STATE), BF),
            vm((n, 4 * sl + 16, STATE), BF),
            vm((n, 4 * sl, STATE), BF),
            vm((n, 4 * sl, STATE), BF),
            vm((n, 4 * sl, STATE), F32),
            vm((n, 8, STATE), F32),
            vm((nx, 2, rows, dim), BF),
            vm((nx, rows, dim), BF),
            vm((nx, rows, dim), BF),
            vm((2, rows, dim), BF),
            vm((rows, dim), BF),
            dma((1,)),
            dma((half, n)),
            dma((1,)),
            dma((half, n)),
            dma((2,)),
            dma((2, n)),
            dma((2,)),
            dma((1 + nx,)),
            dma((2, 2)),
            dma((2,)),
            dma((3,)),
            dma((3,)),
            dma((1,)),
            dma((ncol,)),
            dma((2,)),
            dma((2, ncol)),
            *[vm(v.shape, v.dtype) for v in operands],
            dma((14,)),
        ],
        compiler_params=pltpu.CompilerParams(
            collective_id=0, has_side_effects=True, vmem_limit_bytes=60 * 1024 * 1024
        ),
        name="layer",
    )(*operands)


def solution(mesh):
    n = 8 if mesh.shape["sp"] == 64 else int(round(mesh.shape["sp"] ** 0.5))
    sp_tp = ("sp", "tp")
    return jax.shard_map(
        functools.partial(run_layer, n, mesh.shape["tp"], 4),
        mesh=mesh,
        in_specs=(
            P(sp_tp, None),
            P(),
            P(None, "sp", "tp"),
            P(None, "sp", "tp"),
            P(None, "sp", "tp"),
            P(None, None, "tp"),
            P(None, "tp"),
            P(None, "tp"),
            P(None, None, "tp"),
            P(None, "tp"),
            P("sp", "tp"),
            P("tp"),
            P("tp", "sp"),
            P("tp", "sp"),
        ),
        out_specs=P(sp_tp, None),
        check_vma=False,
    )
```

```python
import functools

import jax
import jax.numpy as jnp
from jax import lax
from jax.experimental import pallas as pl
from jax.experimental.pallas import tpu as pltpu
from jax.sharding import PartitionSpec as P

HEAD = 64
STATE = 128
CH = 128
EDGE = 16
EPS = 1e-05
BF = jnp.bfloat16
F32 = jnp.float32
MESH_IDS = pl.DeviceIdType.MESH


def wide(v):
    return v.astype(F32)


def dot_nt(a, b):
    return lax.dot_general(a, b, (((1,), (1,)), ((), ())), preferred_element_type=F32)


def dot_tn(a, b):
    return lax.dot_general(a, b, (((0,), (0,)), ((), ())), preferred_element_type=F32)


def silu(v):
    return v * jax.nn.sigmoid(v)


def softplus(v):
    return jnp.maximum(v, 0.0) + jnp.log1p(jnp.exp(-jnp.abs(v)))


def layer(
    n,
    tps,
    x_hbm,
    gain_hbm,
    slide_hbm,
    rec_hbm,
    lat_hbm,
    step_hbm,
    ctap_hbm,
    xtap_hbm,
    ltap_hbm,
    rate_hbm,
    spike_hbm,
    lane_hbm,
    cexit_hbm,
    sexit_hbm,
    out_ref,
    abuf,
    w1,
    w2,
    p1,
    p2,
    mixed,
    ycat,
    yacc,
    sb1,
    rb1,
    sb2,
    rb2,
    sb3,
    rb3,
    pre,
    prd,
    obf,
    prx,
    xsend,
    xrecv,
    lrecv,
    s1,
    r1,
    s2,
    r2,
    ps,
    pr,
    asem,
    arem,
    hs,
    hr,
    es,
    er,
    os_,
    or_,
    xs,
    xr,
    x_ref,
    gain_ref,
    slide_ref,
    rec_ref,
    lat_ref,
    step_ref,
    ctap_ref,
    xtap_ref,
    ltap_ref,
    rate_ref,
    spike_ref,
    lane_ref,
    cexit_ref,
    sexit_ref,
    ins,
):
    rows = x_ref.shape[0]
    dim = x_ref.shape[1]
    nx = tps // 2
    length = rows * tps
    half = n // 2
    sl = HEAD // n
    ncol = or_.shape[0]
    wcol = dim // ncol
    sp = lax.axis_index("sp")
    tp = lax.axis_index("tp")
    z = sp // n
    y = sp % n
    cx = tp // 2
    core = tp % 2

    def remote(src, dst, ss, rs, zz, yy, tt):
        return pltpu.make_async_remote_copy(
            src_ref=src,
            dst_ref=dst,
            send_sem=ss,
            recv_sem=rs,
            device_id=(zz * n + yy, tt),
            device_id_type=MESH_IDS,
        )

    given = (
        (x_hbm, x_ref),
        (gain_hbm, gain_ref),
        (slide_hbm, slide_ref),
        (rec_hbm, rec_ref),
        (lat_hbm, lat_ref),
        (step_hbm, step_ref),
        (ctap_hbm, ctap_ref),
        (xtap_hbm, xtap_ref),
        (ltap_hbm, ltap_ref),
        (rate_hbm, rate_ref),
        (spike_hbm, spike_ref),
        (lane_hbm, lane_ref),
        (cexit_hbm, cexit_ref),
        (sexit_hbm, sexit_ref),
    )
    loads = [pltpu.make_async_copy(src, dst, ins.at[i]) for i, (src, dst) in enumerate(given)]
    for load in loads:
        load.start()

    bar = pltpu.get_barrier_semaphore()

    def greet(s, t):
        pl.semaphore_signal(bar, inc=1, device_id=(s, t), device_id_type=MESH_IDS)

    for k in range(1, n):
        greet(z * n + (y + k) % n, tp)
        greet(((z + k) % n) * n + y, tp)
    for k in range(1, tps):
        greet(sp, (tp + k) % tps)
    greet((sp + 1) % (n * n), tp)
    greet((sp + n * n - 1) % (n * n), tp)

    for load in loads:
        load.wait()
    xf = wide(x_ref[...])
    scale = lax.rsqrt(jnp.mean(xf * xf, axis=-1, keepdims=True) + EPS)
    own_rows = pl.ds(pl.multiple_of(EDGE + rows * tp, 16), rows)
    gains = wide(gain_ref[...])
    for j in range(dim // 128):
        cols = slice(128 * j, 128 * j + 128)
        abuf[own_rows, cols] = (xf[:, cols] * scale * gains[j : j + 1, :]).astype(BF)

    @pl.when(sp == 0)
    def _():
        abuf[pl.ds(0, EDGE), :] = jnp.zeros((EDGE, dim), BF)

    @pl.when(sp == n * n - 1)
    def _():
        abuf[pl.ds(EDGE + length, EDGE), :] = jnp.zeros((EDGE, dim), BF)

    for h in range(2):
        cut = slice(16 * h, 16 * h + 16)
        w1[z, y, h, :, 0:128] = rec_ref[1, cut, :]
        w1[z, y, h, :, 128:384] = lat_ref[0, cut, :]
        w1[z, y, h, :, 384:640] = lat_ref[1, cut, :]
        w2[z, y, h, :, 0:128] = slide_ref[0, cut, :]
        w2[z, y, h, :, 128:256] = slide_ref[1, cut, :]
        w2[z, y, h, :, 256:384] = slide_ref[2, cut, :]
        w2[z, y, h, :, 384:512] = rec_ref[0, cut, :]
        w2[z, y, h, :, 512:640] = cexit_ref[cut, :]
        w2[z, y, h, :, 640:768] = sexit_ref[cut, :]

    pl.semaphore_wait(bar, 2 * (n - 1) + (tps - 1) + 2)

    def moved(h, phase, k):
        on_y = (h == 0) == (phase == 1)
        return (z, (y + k + n) % n) if on_y else ((z + k + n) % n, y)

    def piece(h, c, s, d):
        off = -((c + 1) // 2) if c % 2 else c // 2
        return place(h, off, s, d)

    def place(h, off, s, d):
        if h == 0:
            return (z - d * s + n) % n, (y + off + n) % n, 0
        return (z + off + n) % n, (y - d * s + n) % n, 1

    def ring_one(w, ss, rs, qs, qr, rnd, straight):
        def first(h, c, nxt):
            d = 1 if nxt % 2 else -1
            ref = w.at[piece(h, c, 0, 1)]
            zz, yy = moved(h, 1, d)
            return remote(ref, ref, qs.at[rnd], qr.at[rnd, nxt], zz, yy, tp)

        def first_in(c):
            ref = w.at[0, 0]
            remote(ref, ref, qs.at[rnd], qr.at[rnd, c], z, y, tp).wait_recv()

        def second(h, off, c, s, di, d):
            ref = w.at[place(h, off, s, d)]
            zz, yy = moved(h, 2, d)
            return remote(ref, ref, ss.at[0], rs.at[s, c], zz, yy, tp)

        def second_in(c, s):
            ref = w.at[0, 0:2] if s < half else w.at[0, 0]
            remote(ref, ref, ss.at[0], rs.at[s - 1, c], z, y, tp).wait_recv()

        def offset(c):
            return jnp.where(c % 2 == 1, -((c + 1) // 2), c // 2)

        def direct(h, c):
            d = (c + 1) // 2 if c % 2 else -(c // 2)
            ref = w.at[piece(h, 0, 0, 1)]
            zz, yy = moved(h, 1, d)
            return remote(ref, ref, qs.at[rnd], qr.at[rnd, c], zz, yy, tp)

        def spread(lo, hi):
            for c in range(lo, hi):
                for h in range(2):
                    direct(h, c).start()

        def lead(lo, hi):
            for c in range(lo, hi):
                if c > 0:
                    first_in(c)
                for h in range(2):
                    if c == 0:
                        first(h, 0, 1).start()
                        first(h, 0, 2).start()
                    elif c + 2 < n:
                        first(h, c, c + 2).start()

        def start(c):
            if straight and c > 0:
                first_in(c)
            for h in range(2):
                off = -((c + 1) // 2) if c % 2 else c // 2
                for di, d in ((0, 1), (1, -1)):
                    if half > 1 or di == c % 2:
                        second(h, off, c, 0, di, d).start()

        def pass_on(s, c):
            off = offset(c)
            second_in(c, s)
            for h in range(2):
                if s < half - 1:
                    for di, d in ((0, 1), (1, -1)):
                        second(h, off, c, s, di, d).start()
                else:
                    di = c % 2
                    second(h, off, c, s, di, 1 - 2 * di).start()

        def advance(lo, hi):
            while lo < hi:
                s, c = divmod(lo, n)
                if s == 0:
                    start(c)
                    lo += 1
                elif s < half:
                    stop = min(hi, (s + 1) * n)

                    @pl.loop(c, c + stop - lo)
                    def _(cc, s=s):
                        pass_on(s, cc)

                    lo = stop
                else:
                    stop = min(hi, (s + 1) * n)

                    @pl.loop(c, c + stop - lo)
                    def _(cc, s=s):
                        second_in(cc, s)

                    lo = stop

        def drain():
            lead_all = w.at[0, 0 : n - 1]
            remote(lead_all, lead_all, qs.at[rnd], qr.at[rnd, 0], z, y, tp).wait_send()
            ring_all = w.at[0 : n - 1]
            remote(ring_all, ring_all, ss.at[0], rs.at[0, 0], z, y, tp).wait_send()

        return advance, drain, spread, lead

    turns = (half + 1) * n
    ring1, drain1, spread1, _ = ring_one(w1, s1, r1, ps, pr, 0, True)
    ring2, drain2, _, lead2 = ring_one(w2, s2, r2, ps, pr, 1, False)

    def block(t):
        return abuf.at[pl.ds(pl.multiple_of(EDGE + rows * t, 16), rows), :]

    def a_out(k):
        return remote(block(tp), block(tp), asem.at[0], arem.at[k], z, y, ((cx + k) % nx) * 2 + core)

    def a_in(k):
        t = ((cx + nx - k) % nx) * 2 + core
        return remote(block(t), block(t), asem.at[0], arem.at[k], z, y, tp)

    def a_pair(k):
        t = ((cx + nx - k) % nx) * 2 + core
        return remote(block(t), block(t), asem.at[1], arem.at[nx], z, y, cx * 2 + 1 - core)

    def a_wait(blocks, which):
        ref = abuf.at[pl.ds(0, rows * blocks), :]
        return remote(ref, ref, asem.at[which], arem.at[nx], z, y, tp)

    before = abuf.at[pl.ds(0, EDGE), :]
    after = abuf.at[pl.ds(EDGE + length, EDGE), :]
    last_own = abuf.at[pl.ds(EDGE + length - EDGE, EDGE), :]
    first_own = abuf.at[pl.ds(EDGE, EDGE), :]
    down = (sp + n * n - 1) % (n * n)
    up = (sp + 1) % (n * n)
    far = tps - 1

    def edge_next():
        return remote(last_own, before, hs.at[0, 0], hr.at[0], up // n, up % n, far)

    def edge_prev():
        return remote(first_own, after, hs.at[1, 0], hr.at[1], down // n, down % n, 0)

    def edge_share(side, k):
        ref = (before, after)[side]
        return remote(ref, ref, hs.at[side, 1], hr.at[side], z, y, ((far, 0)[side] + k) % tps)

    def edge_in(side):
        ref = (before, after)[side]
        remote(ref, ref, hs.at[side, 1], hr.at[side], z, y, tp).wait_recv()

    def edge_sent(side):
        ref = abuf.at[pl.ds(0, EDGE * (tps - 1)), :]
        remote(ref, ref, hs.at[side, 1], hr.at[side], z, y, tp).wait_send()

    spread1(1, 3)
    ring1(0, 1)
    spread1(3, n)
    for k in range(1, nx):
        a_out(k).start()
    a_pair(0).start()

    @pl.when((tp == far) & (sp < n * n - 1))
    def _():
        edge_next().start()

    @pl.when((tp == 0) & (sp > 0))
    def _():
        edge_prev().start()

    ring1(1, 3)
    lead2(0, 1)
    ring1(n, n + 1)
    ring1(3, 5)
    ring1(n + 1, n + 3)
    ring1(5, n)

    @pl.when((tp == far) & (sp > 0))
    def _():
        edge_in(0)
        for k in range(1, tps):
            edge_share(0, k).start()

    @pl.when((tp == 0) & (sp < n * n - 1))
    def _():
        edge_in(1)
        for k in range(1, tps):
            edge_share(1, k).start()

    lead2(1, 3)
    ring1(n + 3, 2 * n)
    for k in range(1, nx):
        if k != half_way(nx):
            a_in(k).wait_recv()
            a_pair(k).start()
    lead2(3, 5)
    ring1(2 * n, 3 * n)
    a_in(half_way(nx)).wait_recv()
    a_pair(half_way(nx)).start()
    lead2(5, 7)
    ring1(3 * n, 4 * n)
    lead2(7, 8)
    ring2(0, 4)

    a_wait(nx, 1).wait_recv()

    @pl.when((tp != far) & (sp > 0))
    def _():
        edge_in(0)

    @pl.when((tp != 0) & (sp < n * n - 1))
    def _():
        edge_in(1)

    steps = jnp.concatenate([step_ref[0], step_ref[1], jnp.zeros((12, dim), BF)], axis=0)
    raw = dot_nt(steps, abuf[EDGE : EDGE + length, :])[0:8]
    deltas = softplus(wide(raw.astype(BF)))
    spike = spike_ref[...]
    spikes = jnp.concatenate([spike, spike, jnp.zeros((4, length), F32)], axis=0)
    row_id = lax.broadcasted_iota(jnp.int32, (8, 1), 0)
    rates = jnp.zeros((8, 1), F32)
    for k in range(4):
        rates = jnp.where(row_id == k, rate_ref[k // 2 : k // 2 + 1, k % 2 : k % 2 + 1], rates)
    logs = spikes - deltas * rates
    logs = jnp.where(row_id < 4, logs, 0.0)
    lane = lax.broadcasted_iota(jnp.int32, (8, length), 1)
    fsum = logs
    bsum = logs
    shift = 1
    while shift < length:
        fsum = fsum + jnp.where(lane >= shift, pltpu.roll(fsum, shift, axis=1), 0.0)
        bsum = bsum + jnp.where(lane < length - shift, pltpu.roll(bsum, length - shift, axis=1), 0.0)
        shift *= 2
    run = jnp.where(row_id < 2, fsum, bsum)
    total = jnp.where(row_id < 2, fsum[:, length - 1 : length], bsum[:, 0:1])
    weight = jnp.exp(total - run) * deltas
    turned = jnp.concatenate([run, weight, jnp.exp(run), jnp.zeros((CH - 24, length), F32)], axis=0).T

    ring1(4 * n, turns)
    ring2(4, 6)

    def project1(lo, hi):
        w = w1[:, :, :, :, lo:hi].reshape(dim, hi - lo)
        if hi - lo > 128:
            got = jnp.dot(abuf[...], w, preferred_element_type=F32)
        else:
            cut = (length + 2 * EDGE) // 2
            top = jnp.dot(abuf[:cut, :], w, preferred_element_type=F32)
            low_part = jnp.dot(abuf[cut:, :], w, preferred_element_type=F32)
            got = jnp.concatenate([top, low_part], axis=0)
        p1[:, lo:hi] = wide(got.astype(BF))

    tb = 128 if length % 128 == 0 else rows

    def mix(lo):
        if lo == 0:
            taps = wide(xtap_ref[...])
        else:
            at = lo - 128
            taps = wide(ltap_ref[:, at // 256, at % 256 : at % 256 + 128])
        for b in range(length // tb):
            acc = None
            for k in range(5):
                term = p1[EDGE - 2 + k + b * tb : EDGE - 2 + k + (b + 1) * tb, lo : lo + 128] * taps[k : k + 1, :]
                acc = term if acc is None else acc + term
            mixed[b * tb : (b + 1) * tb, lo : lo + 128] = silu(acc).astype(BF)

    project1(0, 512)
    ring2(6, 9)
    project1(512, 640)
    ring2(9, 11)
    for j in range(5):
        mix(128 * j)
    ring2(11, 12)

    low = lax.broadcasted_iota(jnp.int32, (length, CH), 1) < HEAD
    xs_all = wide(mixed[:, 0:128])
    states = []
    for d in range(2):
        w_d = jnp.where(low, turned[:, 8 + 2 * d : 9 + 2 * d], turned[:, 9 + 2 * d : 10 + 2 * d])
        xw = (xs_all * w_d).astype(BF)
        for h in range(2):
            full = dot_tn(xw, mixed[:, 128 + 128 * h : 256 + 128 * h])
            states.append(full[HEAD * h : HEAD * h + HEAD, :])
    decay = jnp.broadcast_to(jnp.exp(total), (8, STATE))

    def packed(parts, dec):
        high = dec.astype(BF)
        rest = dec - wide(high)
        return jnp.concatenate([*parts, wide(high)[0:4], rest[0:4]], axis=0).astype(BF)

    for j in range(n):
        got = packed([s[sl * j : sl * j + sl, :] for s in states], decay)
        sb1[j] = got
    rb1[y] = sb1[y]

    def e1(k):
        yy = (y + k) % n
        return remote(sb1.at[yy], rb1.at[y], es.at[0], er.at[0], z, yy, tp)

    def e2(k):
        return remote(sb2, rb2.at[z], es.at[1], er.at[1], (z + k) % n, y, tp)

    def e3(k):
        yy = (y + k) % n
        return remote(sb3.at[yy], rb3.at[y], es.at[2], er.at[2], z, yy, tp)

    def e_all(which):
        ref = (rb1, rb2, rb3)[which].at[0 : n - 1]
        return remote(ref, ref, es.at[which], er.at[which], z, y, tp)

    for k in range(1, n):
        e1(k).start()

    runs = [run[k : k + 1, :] for k in range(4)]
    dels = [deltas[k : k + 1, :] for k in range(4)]

    def within(h, b):
        scores = dot_nt(
            mixed[b * tb : (b + 1) * tb, 384 + 128 * h : 512 + 128 * h],
            mixed[:, 128 + 128 * h : 256 + 128 * h],
        )
        t_id = lax.broadcasted_iota(jnp.int32, (tb, length), 0) + b * tb
        s_id = lax.broadcasted_iota(jnp.int32, (tb, length), 1)
        part = turned[b * tb : (b + 1) * tb, :]
        gap_f = part[:, h : h + 1] - runs[h]
        gap_b = part[:, 2 + h : 3 + h] - runs[2 + h]
        factor = jnp.where(s_id < t_id, dels[h], jnp.where(s_id > t_id, dels[2 + h], dels[h] + dels[2 + h]))
        decays = jnp.exp(jnp.where(s_id < t_id, gap_f, jnp.where(s_id > t_id, gap_b, 0.0)))
        weights = (scores * decays * factor).astype(BF)
        keep = (lax.broadcasted_iota(jnp.int32, (length, CH), 1) // HEAD) == h
        x_h = jnp.where(keep, xs_all, 0.0).astype(BF)
        got = jnp.dot(weights, x_h, preferred_element_type=F32)
        at = slice(b * tb, (b + 1) * tb)
        yacc[at, :] = got if h == 0 else yacc[at, :] + got

    spots = [(h, b) for h in range(2) for b in range(length // tb)]
    ring2(12, 13)
    for i, (h, b) in enumerate(spots):
        within(h, b)
        ring2(13 + i, 14 + i)

    ring2(19, 22)
    e_all(0).wait_recv()

    carry = [jnp.zeros((sl, STATE), F32) for _ in range(4)]
    prod = [jnp.ones((1, STATE), F32) for _ in range(4)]
    for j in range(n):
        for q in range(4):
            jj = j if q < 2 else n - 1 - j
            blk = wide(rb1[jj])
            pre[jj, sl * q : sl * q + sl, :] = carry[q]
            prd[jj, q : q + 1, :] = prod[q]
            dec = blk[4 * sl + q : 4 * sl + q + 1, :] + blk[4 * sl + 4 + q : 4 * sl + 5 + q, :]
            carry[q] = carry[q] * dec + blk[sl * q : sl * q + sl, :]
            prod[q] = prod[q] * dec
    prods = jnp.concatenate([*prod, jnp.zeros((4, STATE), F32)], axis=0)
    sb2[...] = packed(carry, prods)
    for k in range(1, n):
        e2(k).start()
    ring2(22, 29)
    e_all(1).wait_recv()
    entry = [jnp.zeros((sl, STATE), F32) for _ in range(4)]
    for j in range(n):
        for q in range(4):
            jj = j if q < 2 else n - 1 - j
            blk = wide(rb2[jj])
            dec = blk[4 * sl + q : 4 * sl + q + 1, :] + blk[4 * sl + 4 + q : 4 * sl + 5 + q, :]
            ahead = (jj < z) if q < 2 else (jj > z)
            entry[q] = jnp.where(ahead, entry[q] * dec + blk[sl * q : sl * q + sl, :], entry[q])
    for j in range(n):
        parts = [entry[q] * prd[j, q : q + 1, :] + pre[j, sl * q : sl * q + sl, :] for q in range(4)]
        sb3[j] = jnp.concatenate(parts, axis=0).astype(BF)
    rb3[y] = sb3[y]
    for k in range(1, n):
        e3(k).start()

    ring2(29, turns)

    def project2(lo, hi):
        got = jnp.dot(abuf[...], w2[:, :, :, :, lo:hi].reshape(dim, hi - lo), preferred_element_type=F32)
        p2[:, lo:hi] = wide(got.astype(BF))

    project2(0, 256)
    project2(256, 512)
    p2[:, 128:256] = wide((p2[:, 128:256] * p2[:, 256:384]).astype(BF))
    ctaps = wide(ctap_ref[...])
    for b in range(length // tb):
        acc = None
        for k in range(3):
            term = p2[EDGE - 1 + k + b * tb : EDGE - 1 + k + (b + 1) * tb, 128:256] * ctaps[k : k + 1, :]
            acc = term if acc is None else acc + term
        ycat[b * tb : (b + 1) * tb, 0:128] = (p2[EDGE + b * tb : EDGE + (b + 1) * tb, 0:128] * acc).astype(BF)

    e_all(2).wait_recv()
    blocks = [wide(rb3[j]) for j in range(n)]
    arrived = [
        jnp.concatenate([blk[sl * q : sl * q + sl, :] for blk in blocks], axis=0).astype(BF) for q in range(4)
    ]
    none = jnp.zeros((HEAD, STATE), BF)
    y_all = yacc[...]
    for d in range(2):
        top = jnp.concatenate([arrived[2 * d], none], axis=1)
        bottom = jnp.concatenate([none, arrived[2 * d + 1]], axis=1)
        into = dot_nt(mixed[:, 384:640], jnp.concatenate([top, bottom], axis=0))
        grow = jnp.where(low, turned[:, 16 + 2 * d : 17 + 2 * d], turned[:, 17 + 2 * d : 18 + 2 * d])
        y_all = y_all + into * grow
    g = y_all * silu(p2[EDGE : EDGE + length, 384:512])
    sq = g * g
    mean0 = jnp.sum(jnp.where(low, sq, 0.0), axis=-1, keepdims=True) / HEAD
    mean1 = jnp.sum(jnp.where(low, 0.0, sq), axis=-1, keepdims=True) / HEAD
    inv = jnp.where(low, lax.rsqrt(mean0 + EPS), lax.rsqrt(mean1 + EPS))
    ycat[:, 128:256] = (g * inv * wide(lane_ref[...])).astype(BF)

    def span(c):
        return slice(c * wcol, (c + 1) * wcol)

    def to_pair(c):
        return remote(
            obf.at[:, 1 - core, :, span(c)], prx.at[:, :, span(c)], os_.at[0], or_.at[c], z, y, cx * 2 + 1 - core
        )

    right = (cx + 1) % nx
    left = (cx + nx - 1) % nx
    opposite = (cx + 2) % nx

    def relay(c):
        xx = right if c < ncol // 2 else left
        return remote(
            xsend.at[opposite, :, span(c)], lrecv.at[:, span(c)], xs.at[0], xr.at[0, c], z, y, xx * 2 + core
        )

    def to_owner(c, side):
        xx = (right, left)[side]
        return remote(
            xsend.at[xx, :, span(c)], xrecv.at[side, :, span(c)], xs.at[1], xr.at[1, c], z, y, xx * 2 + core
        )

    def owner_in(c):
        ref = xrecv.at[:, :, span(c)]
        remote(ref, ref, xs.at[1], xr.at[1, c], z, y, tp).wait_recv()

    def chip_sum(xx, c):
        return wide(obf[xx, core, :, span(c)]) + wide(prx[xx, :, span(c)])

    order = [c for pair in zip(range(ncol // 2), range(ncol // 2, ncol)) for c in pair]
    exits = w2[:, :, :, :, 512:768].reshape(dim, 2 * CH)
    for c in order:
        got = dot_nt(ycat[...], exits[c * wcol : (c + 1) * wcol, :])
        obf[:, :, :, span(c)] = got.astype(BF).reshape(nx, 2, rows, wcol)
        to_pair(c).start()
    for c in order:
        to_pair(c).wait_recv()
        xsend[opposite, :, span(c)] = chip_sum(opposite, c).astype(BF)
        relay(c).start()
        side = 1 if c < ncol // 2 else 0
        xx = (right, left)[side]
        xsend[xx, :, span(c)] = chip_sum(xx, c).astype(BF)
        to_owner(c, side).start()
    for c in order:
        relay(c).wait_recv()
        side = 0 if c < ncol // 2 else 1
        xx = (right, left)[side]
        xsend[xx, :, span(c)] = (chip_sum(xx, c) + wide(lrecv[:, span(c)])).astype(BF)
        to_owner(c, side).start()
    drain1()
    drain2()
    for c in order:
        own = chip_sum(cx, c)
        owner_in(c)
        out_ref[:, span(c)] = (own + wide(xrecv[0, :, span(c)]) + wide(xrecv[1, :, span(c)])).astype(BF)

    remote(prx, prx, os_.at[0], or_.at[0], z, y, tp).wait_send()
    relayed = xsend.at[0]
    remote(relayed, relayed, xs.at[0], xr.at[0, 0], z, y, tp).wait_send()
    owned = xsend.at[0:2]
    remote(owned, owned, xs.at[1], xr.at[1, 0], z, y, tp).wait_send()
    for which in range(3):
        e_all(which).wait_send()
    a_wait(nx - 1, 0).wait_send()
    a_wait(nx, 1).wait_send()

    @pl.when((tp == far) & (sp < n * n - 1))
    def _():
        edge_next().wait_send()

    @pl.when((tp == 0) & (sp > 0))
    def _():
        edge_prev().wait_send()

    @pl.when((tp == far) & (sp > 0))
    def _():
        edge_sent(0)

    @pl.when((tp == 0) & (sp < n * n - 1))
    def _():
        edge_sent(1)


def half_way(nx):
    return nx // 2


def run_layer(n, tps, ncol, *args):
    (
        x,
        gain,
        slide,
        rec,
        lat,
        step,
        ctap,
        xtap,
        ltap,
        rate,
        spike,
        lane,
        cexit,
        sexit,
    ) = args
    rows, dim = x.shape
    length = rows * tps
    tall = length + 2 * EDGE
    nx = tps // 2
    half = n // 2
    sl = HEAD // n
    vm = pltpu.VMEM
    dma = pltpu.SemaphoreType.DMA
    vmem = pl.BlockSpec(memory_space=pltpu.VMEM)
    specs = [pl.BlockSpec(memory_space=pltpu.HBM)] * 14
    operands = (
        x,
        gain.reshape(dim // 128, 128),
        slide,
        rec,
        lat,
        step.transpose(1, 2, 0),
        ctap,
        xtap,
        ltap,
        rate,
        spike.T,
        lane.reshape(1, CH),
        cexit.T,
        sexit.T,
    )
    return pl.pallas_call(
        functools.partial(layer, n, tps),
        out_shape=pltpu.VMEM((rows, dim), BF),
        in_specs=specs,
        out_specs=vmem,
        scratch_shapes=[
            vm((tall, dim), BF),
            vm((n, n, 2, 16, 640), BF),
            vm((n, n, 2, 16, 768), BF),
            vm((tall, 640), F32),
            vm((tall, 512), F32),
            vm((length, 640), BF),
            vm((length, 256), BF),
            vm((length, 128), F32),
            vm((n, 4 * sl + 8, STATE), BF),
            vm((n, 4 * sl + 8, STATE), BF),
            vm((4 * sl + 8, STATE), BF),
            vm((n, 4 * sl + 8, STATE), BF),
            vm((n, 4 * sl, STATE), BF),
            vm((n, 4 * sl, STATE), BF),
            vm((n, 4 * sl, STATE), F32),
            vm((n, 8, STATE), F32),
            vm((nx, 2, rows, dim), BF),
            vm((nx, rows, dim), BF),
            vm((nx, rows, dim), BF),
            vm((2, rows, dim), BF),
            vm((rows, dim), BF),
            dma((1,)),
            dma((half, n)),
            dma((1,)),
            dma((half, n)),
            dma((2,)),
            dma((2, n)),
            dma((2,)),
            dma((1 + nx,)),
            dma((2, 2)),
            dma((2,)),
            dma((3,)),
            dma((3,)),
            dma((1,)),
            dma((ncol,)),
            dma((2,)),
            dma((2, ncol)),
            *[vm(v.shape, v.dtype) for v in operands],
            dma((14,)),
        ],
        compiler_params=pltpu.CompilerParams(
            collective_id=0, has_side_effects=True, vmem_limit_bytes=60 * 1024 * 1024
        ),
        name="layer",
    )(*operands)


def solution(mesh):
    n = 8 if mesh.shape["sp"] == 64 else int(round(mesh.shape["sp"] ** 0.5))
    sp_tp = ("sp", "tp")
    return jax.shard_map(
        functools.partial(run_layer, n, mesh.shape["tp"], 4),
        mesh=mesh,
        in_specs=(
            P(sp_tp, None),
            P(),
            P(None, "sp", "tp"),
            P(None, "sp", "tp"),
            P(None, "sp", "tp"),
            P(None, None, "tp"),
            P(None, "tp"),
            P(None, "tp"),
            P(None, None, "tp"),
            P(None, "tp"),
            P("sp", "tp"),
            P("tp"),
            P("tp", "sp"),
            P("tp", "sp"),
        ),
        out_specs=P(sp_tp, None),
        check_vma=False,
    )
```

```python
import functools

import jax
import jax.numpy as jnp
from jax import lax
from jax.experimental import pallas as pl
from jax.experimental.pallas import tpu as pltpu
from jax.sharding import PartitionSpec as P

HEAD = 64
STATE = 128
CH = 128
EDGE = 16
EPS = 1e-05
BF = jnp.bfloat16
F32 = jnp.float32
MESH_IDS = pl.DeviceIdType.MESH


def wide(v):
    return v.astype(F32)


def dot_nt(a, b):
    return lax.dot_general(a, b, (((1,), (1,)), ((), ())), preferred_element_type=F32)


def dot_tn(a, b):
    return lax.dot_general(a, b, (((0,), (0,)), ((), ())), preferred_element_type=F32)


def silu(v):
    return v * jax.nn.sigmoid(v)


def softplus(v):
    return jnp.maximum(v, 0.0) + jnp.log1p(jnp.exp(-jnp.abs(v)))


def layer(
    n,
    tps,
    x_hbm,
    gain_hbm,
    slide_hbm,
    rec_hbm,
    lat_hbm,
    step_hbm,
    ctap_hbm,
    xtap_hbm,
    ltap_hbm,
    rate_hbm,
    spike_hbm,
    lane_hbm,
    cexit_hbm,
    sexit_hbm,
    out_ref,
    abuf,
    w1,
    w2,
    p1,
    p2,
    mixed,
    ycat,
    yacc,
    sb1,
    rb1,
    sb2,
    rb2,
    sb3,
    rb3,
    pre,
    prd,
    obf,
    prx,
    xsend,
    xrecv,
    lrecv,
    s1,
    r1,
    s2,
    r2,
    ps,
    pr,
    asem,
    arem,
    hs,
    hr,
    es,
    er,
    os_,
    or_,
    xs,
    xr,
    x_ref,
    gain_ref,
    slide_ref,
    rec_ref,
    lat_ref,
    step_ref,
    ctap_ref,
    xtap_ref,
    ltap_ref,
    rate_ref,
    spike_ref,
    lane_ref,
    cexit_ref,
    sexit_ref,
    ins,
):
    rows = x_ref.shape[0]
    dim = x_ref.shape[1]
    nx = tps // 2
    length = rows * tps
    half = n // 2
    sl = HEAD // n
    ncol = or_.shape[0]
    wcol = dim // ncol
    sp = lax.axis_index("sp")
    tp = lax.axis_index("tp")
    z = sp // n
    y = sp % n
    cx = tp // 2
    core = tp % 2

    def remote(src, dst, ss, rs, zz, yy, tt):
        return pltpu.make_async_remote_copy(
            src_ref=src,
            dst_ref=dst,
            send_sem=ss,
            recv_sem=rs,
            device_id=(zz * n + yy, tt),
            device_id_type=MESH_IDS,
        )

    given = (
        (x_hbm, x_ref),
        (gain_hbm, gain_ref),
        (slide_hbm, slide_ref),
        (rec_hbm, rec_ref),
        (lat_hbm, lat_ref),
        (step_hbm, step_ref),
        (ctap_hbm, ctap_ref),
        (xtap_hbm, xtap_ref),
        (ltap_hbm, ltap_ref),
        (rate_hbm, rate_ref),
        (spike_hbm, spike_ref),
        (lane_hbm, lane_ref),
        (cexit_hbm, cexit_ref),
        (sexit_hbm, sexit_ref),
    )
    loads = [pltpu.make_async_copy(src, dst, ins.at[i]) for i, (src, dst) in enumerate(given)]
    for load in loads:
        load.start()

    bar = pltpu.get_barrier_semaphore()

    def greet(s, t):
        pl.semaphore_signal(bar, inc=1, device_id=(s, t), device_id_type=MESH_IDS)

    for k in range(1, n):
        greet(z * n + (y + k) % n, tp)
        greet(((z + k) % n) * n + y, tp)
    for k in range(1, tps):
        greet(sp, (tp + k) % tps)
    greet((sp + 1) % (n * n), tp)
    greet((sp + n * n - 1) % (n * n), tp)

    for load in loads:
        load.wait()
    xf = wide(x_ref[...])
    scale = lax.rsqrt(jnp.mean(xf * xf, axis=-1, keepdims=True) + EPS)
    own_rows = pl.ds(pl.multiple_of(EDGE + rows * tp, 16), rows)
    gains = wide(gain_ref[...])
    for j in range(dim // 128):
        cols = slice(128 * j, 128 * j + 128)
        abuf[own_rows, cols] = (xf[:, cols] * scale * gains[j : j + 1, :]).astype(BF)

    @pl.when(sp == 0)
    def _():
        abuf[pl.ds(0, EDGE), :] = jnp.zeros((EDGE, dim), BF)

    @pl.when(sp == n * n - 1)
    def _():
        abuf[pl.ds(EDGE + length, EDGE), :] = jnp.zeros((EDGE, dim), BF)

    for h in range(2):
        cut = slice(16 * h, 16 * h + 16)
        w1[z, y, h, :, 0:128] = rec_ref[1, cut, :]
        w1[z, y, h, :, 128:384] = lat_ref[0, cut, :]
        w1[z, y, h, :, 384:640] = lat_ref[1, cut, :]
        w2[z, y, h, :, 0:128] = slide_ref[0, cut, :]
        w2[z, y, h, :, 128:256] = slide_ref[1, cut, :]
        w2[z, y, h, :, 256:384] = slide_ref[2, cut, :]
        w2[z, y, h, :, 384:512] = rec_ref[0, cut, :]
        w2[z, y, h, :, 512:640] = cexit_ref[cut, :]
        w2[z, y, h, :, 640:768] = sexit_ref[cut, :]

    pl.semaphore_wait(bar, 2 * (n - 1) + (tps - 1) + 2)

    def moved(h, phase, k):
        on_y = (h == 0) == (phase == 1)
        return (z, (y + k + n) % n) if on_y else ((z + k + n) % n, y)

    def piece(h, c, s, d):
        off = -((c + 1) // 2) if c % 2 else c // 2
        return place(h, off, s, d)

    def place(h, off, s, d):
        if h == 0:
            return (z - d * s + n) % n, (y + off + n) % n, 0
        return (z + off + n) % n, (y - d * s + n) % n, 1

    def ring_one(w, ss, rs, qs, qr, rnd, straight):
        def first(h, c, nxt):
            d = 1 if nxt % 2 else -1
            ref = w.at[piece(h, c, 0, 1)]
            zz, yy = moved(h, 1, d)
            return remote(ref, ref, qs.at[rnd], qr.at[rnd, nxt], zz, yy, tp)

        def first_in(c):
            ref = w.at[0, 0]
            remote(ref, ref, qs.at[rnd], qr.at[rnd, c], z, y, tp).wait_recv()

        def second(h, off, c, s, di, d):
            ref = w.at[place(h, off, s, d)]
            zz, yy = moved(h, 2, d)
            return remote(ref, ref, ss.at[0], rs.at[s, c], zz, yy, tp)

        def second_in(c, s):
            ref = w.at[0, 0:2] if s < half else w.at[0, 0]
            remote(ref, ref, ss.at[0], rs.at[s - 1, c], z, y, tp).wait_recv()

        def offset(c):
            return jnp.where(c % 2 == 1, -((c + 1) // 2), c // 2)

        def direct(h, c):
            d = (c + 1) // 2 if c % 2 else -(c // 2)
            ref = w.at[piece(h, 0, 0, 1)]
            zz, yy = moved(h, 1, d)
            return remote(ref, ref, qs.at[rnd], qr.at[rnd, c], zz, yy, tp)

        def spread(lo, hi):
            for c in range(lo, hi):
                for h in range(2):
                    direct(h, c).start()

        def lead(lo, hi):
            for c in range(lo, hi):
                if c > 0:
                    first_in(c)
                for h in range(2):
                    if c == 0:
                        first(h, 0, 1).start()
                        first(h, 0, 2).start()
                    elif c + 2 < n:
                        first(h, c, c + 2).start()

        def start(c):
            if straight and c > 0:
                first_in(c)
            for h in range(2):
                off = -((c + 1) // 2) if c % 2 else c // 2
                for di, d in ((0, 1), (1, -1)):
                    if half > 1 or di == c % 2:
                        second(h, off, c, 0, di, d).start()

        def pass_on(s, c):
            off = offset(c)
            second_in(c, s)
            for h in range(2):
                if s < half - 1:
                    for di, d in ((0, 1), (1, -1)):
                        second(h, off, c, s, di, d).start()
                else:
                    di = c % 2
                    second(h, off, c, s, di, 1 - 2 * di).start()

        def advance(lo, hi):
            while lo < hi:
                s, c = divmod(lo, n)
                if s == 0:
                    start(c)
                    lo += 1
                elif s < half:
                    stop = min(hi, (s + 1) * n)

                    @pl.loop(c, c + stop - lo)
                    def _(cc, s=s):
                        pass_on(s, cc)

                    lo = stop
                else:
                    stop = min(hi, (s + 1) * n)

                    @pl.loop(c, c + stop - lo)
                    def _(cc, s=s):
                        second_in(cc, s)

                    lo = stop

        def drain():
            lead_all = w.at[0, 0 : n - 1]
            remote(lead_all, lead_all, qs.at[rnd], qr.at[rnd, 0], z, y, tp).wait_send()
            ring_all = w.at[0 : n - 1]
            remote(ring_all, ring_all, ss.at[0], rs.at[0, 0], z, y, tp).wait_send()

        return advance, drain, spread, lead

    turns = (half + 1) * n
    ring1, drain1, spread1, _ = ring_one(w1, s1, r1, ps, pr, 0, True)
    ring2, drain2, _, lead2 = ring_one(w2, s2, r2, ps, pr, 1, False)

    def block(t):
        return abuf.at[pl.ds(pl.multiple_of(EDGE + rows * t, 16), rows), :]

    def a_out(k):
        return remote(block(tp), block(tp), asem.at[0], arem.at[k], z, y, ((cx + k) % nx) * 2 + core)

    def a_in(k):
        t = ((cx + nx - k) % nx) * 2 + core
        return remote(block(t), block(t), asem.at[0], arem.at[k], z, y, tp)

    def a_pair(k):
        t = ((cx + nx - k) % nx) * 2 + core
        return remote(block(t), block(t), asem.at[1], arem.at[nx], z, y, cx * 2 + 1 - core)

    def a_wait(blocks, which):
        ref = abuf.at[pl.ds(0, rows * blocks), :]
        return remote(ref, ref, asem.at[which], arem.at[nx], z, y, tp)

    before = abuf.at[pl.ds(0, EDGE), :]
    after = abuf.at[pl.ds(EDGE + length, EDGE), :]
    last_own = abuf.at[pl.ds(EDGE + length - EDGE, EDGE), :]
    first_own = abuf.at[pl.ds(EDGE, EDGE), :]
    down = (sp + n * n - 1) % (n * n)
    up = (sp + 1) % (n * n)
    far = tps - 1

    def edge_next():
        return remote(last_own, before, hs.at[0, 0], hr.at[0], up // n, up % n, far)

    def edge_prev():
        return remote(first_own, after, hs.at[1, 0], hr.at[1], down // n, down % n, 0)

    def edge_share(side, k):
        ref = (before, after)[side]
        return remote(ref, ref, hs.at[side, 1], hr.at[side], z, y, ((far, 0)[side] + k) % tps)

    def edge_in(side):
        ref = (before, after)[side]
        remote(ref, ref, hs.at[side, 1], hr.at[side], z, y, tp).wait_recv()

    def edge_sent(side):
        ref = abuf.at[pl.ds(0, EDGE * (tps - 1)), :]
        remote(ref, ref, hs.at[side, 1], hr.at[side], z, y, tp).wait_send()

    spread1(1, 3)
    ring1(0, 1)
    spread1(3, n)
    for k in range(1, nx):
        a_out(k).start()
    a_pair(0).start()

    @pl.when((tp == far) & (sp < n * n - 1))
    def _():
        edge_next().start()

    @pl.when((tp == 0) & (sp > 0))
    def _():
        edge_prev().start()

    ring1(1, 3)
    lead2(0, 1)
    ring1(n, n + 1)
    ring1(3, 5)
    ring1(n + 1, n + 3)
    ring1(5, n)

    @pl.when((tp == far) & (sp > 0))
    def _():
        edge_in(0)
        for k in range(1, tps):
            edge_share(0, k).start()

    @pl.when((tp == 0) & (sp < n * n - 1))
    def _():
        edge_in(1)
        for k in range(1, tps):
            edge_share(1, k).start()

    lead2(1, 3)
    ring1(n + 3, 2 * n)
    for k in range(1, nx):
        if k != half_way(nx):
            a_in(k).wait_recv()
            a_pair(k).start()
    lead2(3, 5)
    ring1(2 * n, 3 * n)
    a_in(half_way(nx)).wait_recv()
    a_pair(half_way(nx)).start()
    lead2(5, 7)
    ring1(3 * n, 4 * n)
    lead2(7, 8)
    ring2(0, 4)

    a_wait(nx, 1).wait_recv()

    @pl.when((tp != far) & (sp > 0))
    def _():
        edge_in(0)

    @pl.when((tp != 0) & (sp < n * n - 1))
    def _():
        edge_in(1)

    steps = jnp.concatenate([step_ref[0], step_ref[1], jnp.zeros((12, dim), BF)], axis=0)
    raw = dot_nt(steps, abuf[EDGE : EDGE + length, :])[0:8]
    deltas = softplus(wide(raw.astype(BF)))
    spike = spike_ref[...]
    spikes = jnp.concatenate([spike, spike, jnp.zeros((4, length), F32)], axis=0)
    row_id = lax.broadcasted_iota(jnp.int32, (8, 1), 0)
    rates = jnp.zeros((8, 1), F32)
    for k in range(4):
        rates = jnp.where(row_id == k, rate_ref[k // 2 : k // 2 + 1, k % 2 : k % 2 + 1], rates)
    logs = spikes - deltas * rates
    logs = jnp.where(row_id < 4, logs, 0.0)
    lane = lax.broadcasted_iota(jnp.int32, (8, length), 1)
    fsum = logs
    bsum = logs
    shift = 1
    while shift < length:
        fsum = fsum + jnp.where(lane >= shift, pltpu.roll(fsum, shift, axis=1), 0.0)
        bsum = bsum + jnp.where(lane < length - shift, pltpu.roll(bsum, length - shift, axis=1), 0.0)
        shift *= 2
    run = jnp.where(row_id < 2, fsum, bsum)
    total = jnp.where(row_id < 2, fsum[:, length - 1 : length], bsum[:, 0:1])
    weight = jnp.exp(total - run) * deltas
    turned = jnp.concatenate([run, weight, jnp.exp(run), jnp.zeros((CH - 24, length), F32)], axis=0).T

    ring1(4 * n, turns)
    ring2(4, 6)

    def project1(lo, hi):
        w = w1[:, :, :, :, lo:hi].reshape(dim, hi - lo)
        if hi - lo > 128:
            got = jnp.dot(abuf[...], w, preferred_element_type=F32)
        else:
            cut = (length + 2 * EDGE) // 2
            top = jnp.dot(abuf[:cut, :], w, preferred_element_type=F32)
            low_part = jnp.dot(abuf[cut:, :], w, preferred_element_type=F32)
            got = jnp.concatenate([top, low_part], axis=0)
        p1[:, lo:hi] = wide(got.astype(BF))

    tb = 128 if length % 128 == 0 else rows

    def mix(lo):
        if lo == 0:
            taps = wide(xtap_ref[...])
        else:
            at = lo - 128
            taps = wide(ltap_ref[:, at // 256, at % 256 : at % 256 + 128])
        for b in range(length // tb):
            acc = None
            for k in range(5):
                term = p1[EDGE - 2 + k + b * tb : EDGE - 2 + k + (b + 1) * tb, lo : lo + 128] * taps[k : k + 1, :]
                acc = term if acc is None else acc + term
            mixed[b * tb : (b + 1) * tb, lo : lo + 128] = silu(acc).astype(BF)

    project1(0, 512)
    ring2(6, 9)
    project1(512, 640)
    ring2(9, 11)
    for j in range(5):
        mix(128 * j)
    ring2(11, 12)

    low = lax.broadcasted_iota(jnp.int32, (length, CH), 1) < HEAD
    xs_all = wide(mixed[:, 0:128])
    states = []
    for d in range(2):
        w_d = jnp.where(low, turned[:, 8 + 2 * d : 9 + 2 * d], turned[:, 9 + 2 * d : 10 + 2 * d])
        xw = (xs_all * w_d).astype(BF)
        for h in range(2):
            full = dot_tn(xw, mixed[:, 128 + 128 * h : 256 + 128 * h])
            states.append(full[HEAD * h : HEAD * h + HEAD, :])
    decay = jnp.broadcast_to(jnp.exp(total), (8, STATE))

    def packed(parts, dec):
        high = dec.astype(BF)
        rest = dec - wide(high)
        return jnp.concatenate([*parts, wide(high)[0:4], rest[0:4]], axis=0).astype(BF)

    for j in range(n):
        got = packed([s[sl * j : sl * j + sl, :] for s in states], decay)
        sb1[j] = got
    rb1[y] = sb1[y]

    def e1(k):
        yy = (y + k) % n
        return remote(sb1.at[yy], rb1.at[y], es.at[0], er.at[0], z, yy, tp)

    def e2(k):
        return remote(sb2, rb2.at[z], es.at[1], er.at[1], (z + k) % n, y, tp)

    def e3(k):
        yy = (y + k) % n
        return remote(sb3.at[yy], rb3.at[y], es.at[2], er.at[2], z, yy, tp)

    def e_all(which):
        ref = (rb1, rb2, rb3)[which].at[0 : n - 1]
        return remote(ref, ref, es.at[which], er.at[which], z, y, tp)

    for k in range(1, n):
        e1(k).start()

    runs = [run[k : k + 1, :] for k in range(4)]
    dels = [deltas[k : k + 1, :] for k in range(4)]

    def within(h, b):
        scores = dot_nt(
            mixed[b * tb : (b + 1) * tb, 384 + 128 * h : 512 + 128 * h],
            mixed[:, 128 + 128 * h : 256 + 128 * h],
        )
        t_id = lax.broadcasted_iota(jnp.int32, (tb, length), 0) + b * tb
        s_id = lax.broadcasted_iota(jnp.int32, (tb, length), 1)
        part = turned[b * tb : (b + 1) * tb, :]
        gap_f = part[:, h : h + 1] - runs[h]
        gap_b = part[:, 2 + h : 3 + h] - runs[2 + h]
        factor = jnp.where(s_id < t_id, dels[h], jnp.where(s_id > t_id, dels[2 + h], dels[h] + dels[2 + h]))
        decays = jnp.exp(jnp.where(s_id < t_id, gap_f, jnp.where(s_id > t_id, gap_b, 0.0)))
        weights = (scores * decays * factor).astype(BF)
        keep = (lax.broadcasted_iota(jnp.int32, (length, CH), 1) // HEAD) == h
        x_h = jnp.where(keep, xs_all, 0.0).astype(BF)
        got = jnp.dot(weights, x_h, preferred_element_type=F32)
        at = slice(b * tb, (b + 1) * tb)
        yacc[at, :] = got if h == 0 else yacc[at, :] + got

    spots = [(h, b) for h in range(2) for b in range(length // tb)]
    ring2(12, 13)
    for i, (h, b) in enumerate(spots):
        within(h, b)
        ring2(13 + i, 14 + i)

    ring2(19, 22)
    e_all(0).wait_recv()

    carry = [jnp.zeros((sl, STATE), F32) for _ in range(4)]
    prod = [jnp.ones((1, STATE), F32) for _ in range(4)]
    for j in range(n):
        for q in range(4):
            jj = j if q < 2 else n - 1 - j
            blk = wide(rb1[jj])
            pre[jj, sl * q : sl * q + sl, :] = carry[q]
            prd[jj, q : q + 1, :] = prod[q]
            dec = blk[4 * sl + q : 4 * sl + q + 1, :] + blk[4 * sl + 4 + q : 4 * sl + 5 + q, :]
            carry[q] = carry[q] * dec + blk[sl * q : sl * q + sl, :]
            prod[q] = prod[q] * dec
    prods = jnp.concatenate([*prod, jnp.zeros((4, STATE), F32)], axis=0)
    sb2[...] = packed(carry, prods)
    for k in range(1, n):
        e2(k).start()
    ring2(22, 32)
    e_all(1).wait_recv()
    entry = [jnp.zeros((sl, STATE), F32) for _ in range(4)]
    for j in range(n):
        for q in range(4):
            jj = j if q < 2 else n - 1 - j
            blk = wide(rb2[jj])
            dec = blk[4 * sl + q : 4 * sl + q + 1, :] + blk[4 * sl + 4 + q : 4 * sl + 5 + q, :]
            ahead = (jj < z) if q < 2 else (jj > z)
            entry[q] = jnp.where(ahead, entry[q] * dec + blk[sl * q : sl * q + sl, :], entry[q])
    for j in range(n):
        parts = [entry[q] * prd[j, q : q + 1, :] + pre[j, sl * q : sl * q + sl, :] for q in range(4)]
        sb3[j] = jnp.concatenate(parts, axis=0).astype(BF)
    rb3[y] = sb3[y]
    for k in range(1, n):
        e3(k).start()

    ring2(32, turns)

    def project2(lo, hi):
        got = jnp.dot(abuf[...], w2[:, :, :, :, lo:hi].reshape(dim, hi - lo), preferred_element_type=F32)
        p2[:, lo:hi] = wide(got.astype(BF))

    project2(0, 256)
    project2(256, 512)
    p2[:, 128:256] = wide((p2[:, 128:256] * p2[:, 256:384]).astype(BF))
    ctaps = wide(ctap_ref[...])
    for b in range(length // tb):
        acc = None
        for k in range(3):
            term = p2[EDGE - 1 + k + b * tb : EDGE - 1 + k + (b + 1) * tb, 128:256] * ctaps[k : k + 1, :]
            acc = term if acc is None else acc + term
        ycat[b * tb : (b + 1) * tb, 0:128] = (p2[EDGE + b * tb : EDGE + (b + 1) * tb, 0:128] * acc).astype(BF)

    e_all(2).wait_recv()
    blocks = [wide(rb3[j]) for j in range(n)]
    arrived = [
        jnp.concatenate([blk[sl * q : sl * q + sl, :] for blk in blocks], axis=0).astype(BF) for q in range(4)
    ]
    none = jnp.zeros((HEAD, STATE), BF)
    y_all = yacc[...]
    for d in range(2):
        top = jnp.concatenate([arrived[2 * d], none], axis=1)
        bottom = jnp.concatenate([none, arrived[2 * d + 1]], axis=1)
        into = dot_nt(mixed[:, 384:640], jnp.concatenate([top, bottom], axis=0))
        grow = jnp.where(low, turned[:, 16 + 2 * d : 17 + 2 * d], turned[:, 17 + 2 * d : 18 + 2 * d])
        y_all = y_all + into * grow
    g = y_all * silu(p2[EDGE : EDGE + length, 384:512])
    sq = g * g
    mean0 = jnp.sum(jnp.where(low, sq, 0.0), axis=-1, keepdims=True) / HEAD
    mean1 = jnp.sum(jnp.where(low, 0.0, sq), axis=-1, keepdims=True) / HEAD
    inv = jnp.where(low, lax.rsqrt(mean0 + EPS), lax.rsqrt(mean1 + EPS))
    ycat[:, 128:256] = (g * inv * wide(lane_ref[...])).astype(BF)

    def span(c):
        return slice(c * wcol, (c + 1) * wcol)

    def to_pair(c):
        return remote(
            obf.at[:, 1 - core, :, span(c)], prx.at[:, :, span(c)], os_.at[0], or_.at[c], z, y, cx * 2 + 1 - core
        )

    right = (cx + 1) % nx
    left = (cx + nx - 1) % nx
    opposite = (cx + 2) % nx

    def relay(c):
        xx = right if c < ncol // 2 else left
        return remote(
            xsend.at[opposite, :, span(c)], lrecv.at[:, span(c)], xs.at[0], xr.at[0, c], z, y, xx * 2 + core
        )

    def to_owner(c, side):
        xx = (right, left)[side]
        return remote(
            xsend.at[xx, :, span(c)], xrecv.at[side, :, span(c)], xs.at[1], xr.at[1, c], z, y, xx * 2 + core
        )

    def owner_in(c):
        ref = xrecv.at[:, :, span(c)]
        remote(ref, ref, xs.at[1], xr.at[1, c], z, y, tp).wait_recv()

    def chip_sum(xx, c):
        return wide(obf[xx, core, :, span(c)]) + wide(prx[xx, :, span(c)])

    order = [c for pair in zip(range(ncol // 2), range(ncol // 2, ncol)) for c in pair]
    exits = w2[:, :, :, :, 512:768].reshape(dim, 2 * CH)
    for c in order:
        got = dot_nt(ycat[...], exits[c * wcol : (c + 1) * wcol, :])
        obf[:, :, :, span(c)] = got.astype(BF).reshape(nx, 2, rows, wcol)
        to_pair(c).start()
    for c in order:
        to_pair(c).wait_recv()
        xsend[opposite, :, span(c)] = chip_sum(opposite, c).astype(BF)
        relay(c).start()
        side = 1 if c < ncol // 2 else 0
        xx = (right, left)[side]
        xsend[xx, :, span(c)] = chip_sum(xx, c).astype(BF)
        to_owner(c, side).start()
    for c in order:
        relay(c).wait_recv()
        side = 0 if c < ncol // 2 else 1
        xx = (right, left)[side]
        xsend[xx, :, span(c)] = (chip_sum(xx, c) + wide(lrecv[:, span(c)])).astype(BF)
        to_owner(c, side).start()
    drain1()
    drain2()
    for c in order:
        own = chip_sum(cx, c)
        owner_in(c)
        out_ref[:, span(c)] = (own + wide(xrecv[0, :, span(c)]) + wide(xrecv[1, :, span(c)])).astype(BF)

    remote(prx, prx, os_.at[0], or_.at[0], z, y, tp).wait_send()
    relayed = xsend.at[0]
    remote(relayed, relayed, xs.at[0], xr.at[0, 0], z, y, tp).wait_send()
    owned = xsend.at[0:2]
    remote(owned, owned, xs.at[1], xr.at[1, 0], z, y, tp).wait_send()
    for which in range(3):
        e_all(which).wait_send()
    a_wait(nx - 1, 0).wait_send()
    a_wait(nx, 1).wait_send()

    @pl.when((tp == far) & (sp < n * n - 1))
    def _():
        edge_next().wait_send()

    @pl.when((tp == 0) & (sp > 0))
    def _():
        edge_prev().wait_send()

    @pl.when((tp == far) & (sp > 0))
    def _():
        edge_sent(0)

    @pl.when((tp == 0) & (sp < n * n - 1))
    def _():
        edge_sent(1)


def half_way(nx):
    return nx // 2


def run_layer(n, tps, ncol, *args):
    (
        x,
        gain,
        slide,
        rec,
        lat,
        step,
        ctap,
        xtap,
        ltap,
        rate,
        spike,
        lane,
        cexit,
        sexit,
    ) = args
    rows, dim = x.shape
    length = rows * tps
    tall = length + 2 * EDGE
    nx = tps // 2
    half = n // 2
    sl = HEAD // n
    vm = pltpu.VMEM
    dma = pltpu.SemaphoreType.DMA
    vmem = pl.BlockSpec(memory_space=pltpu.VMEM)
    specs = [pl.BlockSpec(memory_space=pltpu.HBM)] * 14
    operands = (
        x,
        gain.reshape(dim // 128, 128),
        slide,
        rec,
        lat,
        step.transpose(1, 2, 0),
        ctap,
        xtap,
        ltap,
        rate,
        spike.T,
        lane.reshape(1, CH),
        cexit.T,
        sexit.T,
    )
    return pl.pallas_call(
        functools.partial(layer, n, tps),
        out_shape=pltpu.VMEM((rows, dim), BF),
        in_specs=specs,
        out_specs=vmem,
        scratch_shapes=[
            vm((tall, dim), BF),
            vm((n, n, 2, 16, 640), BF),
            vm((n, n, 2, 16, 768), BF),
            vm((tall, 640), F32),
            vm((tall, 512), F32),
            vm((length, 640), BF),
            vm((length, 256), BF),
            vm((length, 128), F32),
            vm((n, 4 * sl + 8, STATE), BF),
            vm((n, 4 * sl + 8, STATE), BF),
            vm((4 * sl + 8, STATE), BF),
            vm((n, 4 * sl + 8, STATE), BF),
            vm((n, 4 * sl, STATE), BF),
            vm((n, 4 * sl, STATE), BF),
            vm((n, 4 * sl, STATE), F32),
            vm((n, 8, STATE), F32),
            vm((nx, 2, rows, dim), BF),
            vm((nx, rows, dim), BF),
            vm((nx, rows, dim), BF),
            vm((2, rows, dim), BF),
            vm((rows, dim), BF),
            dma((1,)),
            dma((half, n)),
            dma((1,)),
            dma((half, n)),
            dma((2,)),
            dma((2, n)),
            dma((2,)),
            dma((1 + nx,)),
            dma((2, 2)),
            dma((2,)),
            dma((3,)),
            dma((3,)),
            dma((1,)),
            dma((ncol,)),
            dma((2,)),
            dma((2, ncol)),
            *[vm(v.shape, v.dtype) for v in operands],
            dma((14,)),
        ],
        compiler_params=pltpu.CompilerParams(
            collective_id=0, has_side_effects=True, vmem_limit_bytes=60 * 1024 * 1024
        ),
        name="layer",
    )(*operands)


def solution(mesh):
    n = 8 if mesh.shape["sp"] == 64 else int(round(mesh.shape["sp"] ** 0.5))
    sp_tp = ("sp", "tp")
    return jax.shard_map(
        functools.partial(run_layer, n, mesh.shape["tp"], 4),
        mesh=mesh,
        in_specs=(
            P(sp_tp, None),
            P(),
            P(None, "sp", "tp"),
            P(None, "sp", "tp"),
            P(None, "sp", "tp"),
            P(None, None, "tp"),
            P(None, "tp"),
            P(None, "tp"),
            P(None, None, "tp"),
            P(None, "tp"),
            P("sp", "tp"),
            P("tp"),
            P("tp", "sp"),
            P("tp", "sp"),
        ),
        out_specs=P(sp_tp, None),
        check_vma=False,
    )
```

```python
import functools

import jax
import jax.numpy as jnp
from jax import lax
from jax.experimental import pallas as pl
from jax.experimental.pallas import tpu as pltpu
from jax.sharding import PartitionSpec as P

HEAD = 64
STATE = 128
CH = 128
EDGE = 16
EPS = 1e-05
BF = jnp.bfloat16
F32 = jnp.float32
MESH_IDS = pl.DeviceIdType.MESH


def wide(v):
    return v.astype(F32)


def dot_nt(a, b):
    return lax.dot_general(a, b, (((1,), (1,)), ((), ())), preferred_element_type=F32)


def dot_tn(a, b):
    return lax.dot_general(a, b, (((0,), (0,)), ((), ())), preferred_element_type=F32)


def silu(v):
    return v * jax.nn.sigmoid(v)


def softplus(v):
    return jnp.maximum(v, 0.0) + jnp.log1p(jnp.exp(-jnp.abs(v)))


def layer(
    n,
    tps,
    x_hbm,
    gain_hbm,
    slide_hbm,
    rec_hbm,
    lat_hbm,
    step_hbm,
    ctap_hbm,
    xtap_hbm,
    ltap_hbm,
    rate_hbm,
    spike_hbm,
    lane_hbm,
    cexit_hbm,
    sexit_hbm,
    out_ref,
    abuf,
    w1,
    w2,
    p1,
    p2,
    mixed,
    ycat,
    yacc,
    sb1,
    rb1,
    sb2,
    rb2,
    sb3,
    rb3,
    pre,
    prd,
    obf,
    prx,
    xsend,
    xrecv,
    lrecv,
    s1,
    r1,
    s2,
    r2,
    ps,
    pr,
    asem,
    arem,
    hs,
    hr,
    es,
    er,
    os_,
    or_,
    xs,
    xr,
    x_ref,
    gain_ref,
    slide_ref,
    rec_ref,
    lat_ref,
    step_ref,
    ctap_ref,
    xtap_ref,
    ltap_ref,
    rate_ref,
    spike_ref,
    lane_ref,
    cexit_ref,
    sexit_ref,
    ins,
):
    rows = x_ref.shape[0]
    dim = x_ref.shape[1]
    nx = tps // 2
    length = rows * tps
    half = n // 2
    sl = HEAD // n
    ncol = or_.shape[0]
    wcol = dim // ncol
    sp = lax.axis_index("sp")
    tp = lax.axis_index("tp")
    z = sp // n
    y = sp % n
    cx = tp // 2
    core = tp % 2

    def remote(src, dst, ss, rs, zz, yy, tt):
        return pltpu.make_async_remote_copy(
            src_ref=src,
            dst_ref=dst,
            send_sem=ss,
            recv_sem=rs,
            device_id=(zz * n + yy, tt),
            device_id_type=MESH_IDS,
        )

    given = (
        (x_hbm, x_ref),
        (gain_hbm, gain_ref),
        (slide_hbm, slide_ref),
        (rec_hbm, rec_ref),
        (lat_hbm, lat_ref),
        (step_hbm, step_ref),
        (ctap_hbm, ctap_ref),
        (xtap_hbm, xtap_ref),
        (ltap_hbm, ltap_ref),
        (rate_hbm, rate_ref),
        (spike_hbm, spike_ref),
        (lane_hbm, lane_ref),
        (cexit_hbm, cexit_ref),
        (sexit_hbm, sexit_ref),
    )
    loads = [pltpu.make_async_copy(src, dst, ins.at[i]) for i, (src, dst) in enumerate(given)]
    for load in loads:
        load.start()

    bar = pltpu.get_barrier_semaphore()

    def greet(s, t):
        pl.semaphore_signal(bar, inc=1, device_id=(s, t), device_id_type=MESH_IDS)

    for k in range(1, n):
        greet(z * n + (y + k) % n, tp)
        greet(((z + k) % n) * n + y, tp)
    for k in range(1, tps):
        greet(sp, (tp + k) % tps)
    greet((sp + 1) % (n * n), tp)
    greet((sp + n * n - 1) % (n * n), tp)

    for load in loads:
        load.wait()
    xf = wide(x_ref[...])
    scale = lax.rsqrt(jnp.mean(xf * xf, axis=-1, keepdims=True) + EPS)
    own_rows = pl.ds(pl.multiple_of(EDGE + rows * tp, 16), rows)
    gains = wide(gain_ref[...])
    for j in range(dim // 128):
        cols = slice(128 * j, 128 * j + 128)
        abuf[own_rows, cols] = (xf[:, cols] * scale * gains[j : j + 1, :]).astype(BF)

    @pl.when(sp == 0)
    def _():
        abuf[pl.ds(0, EDGE), :] = jnp.zeros((EDGE, dim), BF)

    @pl.when(sp == n * n - 1)
    def _():
        abuf[pl.ds(EDGE + length, EDGE), :] = jnp.zeros((EDGE, dim), BF)

    for h in range(2):
        cut = slice(16 * h, 16 * h + 16)
        w1[z, y, h, :, 0:128] = rec_ref[1, cut, :]
        w1[z, y, h, :, 128:384] = lat_ref[0, cut, :]
        w1[z, y, h, :, 384:640] = lat_ref[1, cut, :]
        w2[z, y, h, :, 0:128] = slide_ref[0, cut, :]
        w2[z, y, h, :, 128:256] = slide_ref[1, cut, :]
        w2[z, y, h, :, 256:384] = slide_ref[2, cut, :]
        w2[z, y, h, :, 384:512] = rec_ref[0, cut, :]
        w2[z, y, h, :, 512:640] = cexit_ref[cut, :]
        w2[z, y, h, :, 640:768] = sexit_ref[cut, :]

    pl.semaphore_wait(bar, 2 * (n - 1) + (tps - 1) + 2)

    def moved(h, phase, k):
        on_y = (h == 0) == (phase == 1)
        return (z, (y + k + n) % n) if on_y else ((z + k + n) % n, y)

    def piece(h, c, s, d):
        off = -((c + 1) // 2) if c % 2 else c // 2
        return place(h, off, s, d)

    def place(h, off, s, d):
        if h == 0:
            return (z - d * s + n) % n, (y + off + n) % n, 0
        return (z + off + n) % n, (y - d * s + n) % n, 1

    def ring_one(w, ss, rs, qs, qr, rnd, straight):
        def first(h, c, nxt):
            d = 1 if nxt % 2 else -1
            ref = w.at[piece(h, c, 0, 1)]
            zz, yy = moved(h, 1, d)
            return remote(ref, ref, qs.at[rnd], qr.at[rnd, nxt], zz, yy, tp)

        def first_in(c):
            ref = w.at[0, 0]
            remote(ref, ref, qs.at[rnd], qr.at[rnd, c], z, y, tp).wait_recv()

        def second(h, off, c, s, di, d):
            ref = w.at[place(h, off, s, d)]
            zz, yy = moved(h, 2, d)
            return remote(ref, ref, ss.at[0], rs.at[s, c], zz, yy, tp)

        def second_in(c, s):
            ref = w.at[0, 0:2] if s < half else w.at[0, 0]
            remote(ref, ref, ss.at[0], rs.at[s - 1, c], z, y, tp).wait_recv()

        def offset(c):
            return jnp.where(c % 2 == 1, -((c + 1) // 2), c // 2)

        def direct(h, c):
            d = (c + 1) // 2 if c % 2 else -(c // 2)
            ref = w.at[piece(h, 0, 0, 1)]
            zz, yy = moved(h, 1, d)
            return remote(ref, ref, qs.at[rnd], qr.at[rnd, c], zz, yy, tp)

        def spread(lo, hi):
            for c in range(lo, hi):
                for h in range(2):
                    direct(h, c).start()

        def lead(lo, hi):
            for c in range(lo, hi):
                if c > 0:
                    first_in(c)
                for h in range(2):
                    if c == 0:
                        first(h, 0, 1).start()
                        first(h, 0, 2).start()
                    elif c + 2 < n:
                        first(h, c, c + 2).start()

        def start(c):
            if straight and c > 0:
                first_in(c)
            for h in range(2):
                off = -((c + 1) // 2) if c % 2 else c // 2
                for di, d in ((0, 1), (1, -1)):
                    if half > 1 or di == c % 2:
                        second(h, off, c, 0, di, d).start()

        def pass_on(s, c):
            off = offset(c)
            second_in(c, s)
            for h in range(2):
                if s < half - 1:
                    for di, d in ((0, 1), (1, -1)):
                        second(h, off, c, s, di, d).start()
                else:
                    di = c % 2
                    second(h, off, c, s, di, 1 - 2 * di).start()

        def advance(lo, hi):
            while lo < hi:
                s, c = divmod(lo, n)
                if s == 0:
                    start(c)
                    lo += 1
                elif s < half:
                    stop = min(hi, (s + 1) * n)

                    @pl.loop(c, c + stop - lo)
                    def _(cc, s=s):
                        pass_on(s, cc)

                    lo = stop
                else:
                    stop = min(hi, (s + 1) * n)

                    @pl.loop(c, c + stop - lo)
                    def _(cc, s=s):
                        second_in(cc, s)

                    lo = stop

        def drain():
            lead_all = w.at[0, 0 : n - 1]
            remote(lead_all, lead_all, qs.at[rnd], qr.at[rnd, 0], z, y, tp).wait_send()
            ring_all = w.at[0 : n - 1]
            remote(ring_all, ring_all, ss.at[0], rs.at[0, 0], z, y, tp).wait_send()

        return advance, drain, spread, lead

    turns = (half + 1) * n
    ring1, drain1, spread1, _ = ring_one(w1, s1, r1, ps, pr, 0, True)
    ring2, drain2, _, lead2 = ring_one(w2, s2, r2, ps, pr, 1, False)

    def block(t):
        return abuf.at[pl.ds(pl.multiple_of(EDGE + rows * t, 16), rows), :]

    def a_out(k):
        return remote(block(tp), block(tp), asem.at[0], arem.at[k], z, y, ((cx + k) % nx) * 2 + core)

    def a_in(k):
        t = ((cx + nx - k) % nx) * 2 + core
        return remote(block(t), block(t), asem.at[0], arem.at[k], z, y, tp)

    def a_pair(k):
        t = ((cx + nx - k) % nx) * 2 + core
        return remote(block(t), block(t), asem.at[1], arem.at[nx], z, y, cx * 2 + 1 - core)

    def a_wait(blocks, which):
        ref = abuf.at[pl.ds(0, rows * blocks), :]
        return remote(ref, ref, asem.at[which], arem.at[nx], z, y, tp)

    before = abuf.at[pl.ds(0, EDGE), :]
    after = abuf.at[pl.ds(EDGE + length, EDGE), :]
    last_own = abuf.at[pl.ds(EDGE + length - EDGE, EDGE), :]
    first_own = abuf.at[pl.ds(EDGE, EDGE), :]
    down = (sp + n * n - 1) % (n * n)
    up = (sp + 1) % (n * n)
    far = tps - 1

    def edge_next():
        return remote(last_own, before, hs.at[0, 0], hr.at[0], up // n, up % n, far)

    def edge_prev():
        return remote(first_own, after, hs.at[1, 0], hr.at[1], down // n, down % n, 0)

    def edge_share(side, k):
        ref = (before, after)[side]
        return remote(ref, ref, hs.at[side, 1], hr.at[side], z, y, ((far, 0)[side] + k) % tps)

    def edge_in(side):
        ref = (before, after)[side]
        remote(ref, ref, hs.at[side, 1], hr.at[side], z, y, tp).wait_recv()

    def edge_sent(side):
        ref = abuf.at[pl.ds(0, EDGE * (tps - 1)), :]
        remote(ref, ref, hs.at[side, 1], hr.at[side], z, y, tp).wait_send()

    spread1(1, 3)
    ring1(0, 1)
    spread1(3, n)
    for k in range(1, nx):
        a_out(k).start()
    a_pair(0).start()

    @pl.when((tp == far) & (sp < n * n - 1))
    def _():
        edge_next().start()

    @pl.when((tp == 0) & (sp > 0))
    def _():
        edge_prev().start()

    ring1(1, 3)
    lead2(0, 1)
    ring1(n, n + 1)
    ring1(3, 5)
    ring1(n + 1, n + 3)
    ring1(5, n)

    @pl.when((tp == far) & (sp > 0))
    def _():
        edge_in(0)
        for k in range(1, tps):
            edge_share(0, k).start()

    @pl.when((tp == 0) & (sp < n * n - 1))
    def _():
        edge_in(1)
        for k in range(1, tps):
            edge_share(1, k).start()

    lead2(1, 3)
    ring1(n + 3, 2 * n)
    for k in range(1, nx):
        if k != half_way(nx):
            a_in(k).wait_recv()
            a_pair(k).start()
    lead2(3, 5)
    ring1(2 * n, 3 * n)
    a_in(half_way(nx)).wait_recv()
    a_pair(half_way(nx)).start()
    lead2(5, 7)
    ring1(3 * n, 4 * n)
    lead2(7, 8)
    ring2(0, 4)

    a_wait(nx, 1).wait_recv()

    @pl.when((tp != far) & (sp > 0))
    def _():
        edge_in(0)

    @pl.when((tp != 0) & (sp < n * n - 1))
    def _():
        edge_in(1)

    steps = jnp.concatenate([step_ref[0], step_ref[1], jnp.zeros((12, dim), BF)], axis=0)
    raw = dot_nt(steps, abuf[EDGE : EDGE + length, :])[0:8]
    deltas = softplus(wide(raw.astype(BF)))
    spike = spike_ref[...]
    spikes = jnp.concatenate([spike, spike, jnp.zeros((4, length), F32)], axis=0)
    row_id = lax.broadcasted_iota(jnp.int32, (8, 1), 0)
    rates = jnp.zeros((8, 1), F32)
    for k in range(4):
        rates = jnp.where(row_id == k, rate_ref[k // 2 : k // 2 + 1, k % 2 : k % 2 + 1], rates)
    logs = spikes - deltas * rates
    logs = jnp.where(row_id < 4, logs, 0.0)
    lane = lax.broadcasted_iota(jnp.int32, (8, length), 1)
    fsum = logs
    bsum = logs
    shift = 1
    while shift < length:
        fsum = fsum + jnp.where(lane >= shift, pltpu.roll(fsum, shift, axis=1), 0.0)
        bsum = bsum + jnp.where(lane < length - shift, pltpu.roll(bsum, length - shift, axis=1), 0.0)
        shift *= 2
    run = jnp.where(row_id < 2, fsum, bsum)
    total = jnp.where(row_id < 2, fsum[:, length - 1 : length], bsum[:, 0:1])
    weight = jnp.exp(total - run) * deltas
    turned = jnp.concatenate([run, weight, jnp.exp(run), jnp.zeros((CH - 24, length), F32)], axis=0).T

    ring1(4 * n, turns)
    ring2(4, 6)

    def project1(lo, hi):
        w = w1[:, :, :, :, lo:hi].reshape(dim, hi - lo)
        if hi - lo > 128:
            got = jnp.dot(abuf[...], w, preferred_element_type=F32)
        else:
            cut = (length + 2 * EDGE) // 2
            top = jnp.dot(abuf[:cut, :], w, preferred_element_type=F32)
            low_part = jnp.dot(abuf[cut:, :], w, preferred_element_type=F32)
            got = jnp.concatenate([top, low_part], axis=0)
        p1[:, lo:hi] = wide(got.astype(BF))

    tb = 128 if length % 128 == 0 else rows

    def mix(lo):
        if lo == 0:
            taps = wide(xtap_ref[...])
        else:
            at = lo - 128
            taps = wide(ltap_ref[:, at // 256, at % 256 : at % 256 + 128])
        for b in range(length // tb):
            acc = None
            for k in range(5):
                term = p1[EDGE - 2 + k + b * tb : EDGE - 2 + k + (b + 1) * tb, lo : lo + 128] * taps[k : k + 1, :]
                acc = term if acc is None else acc + term
            mixed[b * tb : (b + 1) * tb, lo : lo + 128] = silu(acc).astype(BF)

    project1(0, 512)
    ring2(6, 9)
    project1(512, 640)
    ring2(9, 11)
    for j in range(5):
        mix(128 * j)
    ring2(11, 12)

    low = lax.broadcasted_iota(jnp.int32, (length, CH), 1) < HEAD
    xs_all = wide(mixed[:, 0:128])
    states = []
    for d in range(2):
        w_d = jnp.where(low, turned[:, 8 + 2 * d : 9 + 2 * d], turned[:, 9 + 2 * d : 10 + 2 * d])
        xw = (xs_all * w_d).astype(BF)
        for h in range(2):
            full = dot_tn(xw, mixed[:, 128 + 128 * h : 256 + 128 * h])
            states.append(full[HEAD * h : HEAD * h + HEAD, :])
    decay = jnp.broadcast_to(jnp.exp(total), (8, STATE))

    def packed(parts, dec):
        high = dec.astype(BF)
        rest = dec - wide(high)
        return jnp.concatenate([*parts, wide(high)[0:4], rest[0:4]], axis=0).astype(BF)

    for j in range(n):
        got = packed([s[sl * j : sl * j + sl, :] for s in states], decay)
        sb1[j] = got
    rb1[y] = sb1[y]

    def e1(k):
        yy = (y + k) % n
        return remote(sb1.at[yy], rb1.at[y], es.at[0], er.at[0], z, yy, tp)

    def e2(k):
        return remote(sb2, rb2.at[z], es.at[1], er.at[1], (z + k) % n, y, tp)

    def e3(k):
        yy = (y + k) % n
        return remote(sb3.at[yy], rb3.at[y], es.at[2], er.at[2], z, yy, tp)

    def e_all(which):
        ref = (rb1, rb2, rb3)[which].at[0 : n - 1]
        return remote(ref, ref, es.at[which], er.at[which], z, y, tp)

    for k in range(1, n):
        e1(k).start()

    runs = [run[k : k + 1, :] for k in range(4)]
    dels = [deltas[k : k + 1, :] for k in range(4)]

    def within(h, b):
        scores = dot_nt(
            mixed[b * tb : (b + 1) * tb, 384 + 128 * h : 512 + 128 * h],
            mixed[:, 128 + 128 * h : 256 + 128 * h],
        )
        t_id = lax.broadcasted_iota(jnp.int32, (tb, length), 0) + b * tb
        s_id = lax.broadcasted_iota(jnp.int32, (tb, length), 1)
        part = turned[b * tb : (b + 1) * tb, :]
        gap_f = part[:, h : h + 1] - runs[h]
        gap_b = part[:, 2 + h : 3 + h] - runs[2 + h]
        factor = jnp.where(s_id < t_id, dels[h], jnp.where(s_id > t_id, dels[2 + h], dels[h] + dels[2 + h]))
        decays = jnp.exp(jnp.where(s_id < t_id, gap_f, jnp.where(s_id > t_id, gap_b, 0.0)))
        weights = (scores * decays * factor).astype(BF)
        keep = (lax.broadcasted_iota(jnp.int32, (length, CH), 1) // HEAD) == h
        x_h = jnp.where(keep, xs_all, 0.0).astype(BF)
        got = jnp.dot(weights, x_h, preferred_element_type=F32)
        at = slice(b * tb, (b + 1) * tb)
        yacc[at, :] = got if h == 0 else yacc[at, :] + got

    spots = [(h, b) for h in range(2) for b in range(length // tb)]
    ring2(12, 13)
    for i, (h, b) in enumerate(spots):
        within(h, b)
        ring2(13 + i, 14 + i)

    ring2(19, 22)
    e_all(0).wait_recv()

    carry = [jnp.zeros((sl, STATE), F32) for _ in range(4)]
    prod = [jnp.ones((1, STATE), F32) for _ in range(4)]
    for j in range(n):
        for q in range(4):
            jj = j if q < 2 else n - 1 - j
            blk = wide(rb1[jj])
            pre[jj, sl * q : sl * q + sl, :] = carry[q]
            prd[jj, q : q + 1, :] = prod[q]
            dec = blk[4 * sl + q : 4 * sl + q + 1, :] + blk[4 * sl + 4 + q : 4 * sl + 5 + q, :]
            carry[q] = carry[q] * dec + blk[sl * q : sl * q + sl, :]
            prod[q] = prod[q] * dec
    prods = jnp.concatenate([*prod, jnp.zeros((4, STATE), F32)], axis=0)
    sb2[...] = packed(carry, prods)
    for k in range(1, n):
        e2(k).start()
    ring2(22, 32)
    e_all(1).wait_recv()
    entry = [jnp.zeros((sl, STATE), F32) for _ in range(4)]
    for j in range(n):
        for q in range(4):
            jj = j if q < 2 else n - 1 - j
            blk = wide(rb2[jj])
            dec = blk[4 * sl + q : 4 * sl + q + 1, :] + blk[4 * sl + 4 + q : 4 * sl + 5 + q, :]
            ahead = (jj < z) if q < 2 else (jj > z)
            entry[q] = jnp.where(ahead, entry[q] * dec + blk[sl * q : sl * q + sl, :], entry[q])
    for j in range(n):
        parts = [entry[q] * prd[j, q : q + 1, :] + pre[j, sl * q : sl * q + sl, :] for q in range(4)]
        sb3[j] = jnp.concatenate(parts, axis=0).astype(BF)
    rb3[y] = sb3[y]
    for k in range(1, n):
        e3(k).start()

    ring2(32, turns)

    def project2(lo, hi):
        got = jnp.dot(abuf[...], w2[:, :, :, :, lo:hi].reshape(dim, hi - lo), preferred_element_type=F32)
        p2[:, lo:hi] = wide(got.astype(BF))

    project2(0, 256)
    project2(256, 512)
    p2[:, 128:256] = wide((p2[:, 128:256] * p2[:, 256:384]).astype(BF))
    ctaps = wide(ctap_ref[...])
    for b in range(length // tb):
        acc = None
        for k in range(3):
            term = p2[EDGE - 1 + k + b * tb : EDGE - 1 + k + (b + 1) * tb, 128:256] * ctaps[k : k + 1, :]
            acc = term if acc is None else acc + term
        ycat[b * tb : (b + 1) * tb, 0:128] = (p2[EDGE + b * tb : EDGE + (b + 1) * tb, 0:128] * acc).astype(BF)

    e_all(2).wait_recv()
    blocks = [wide(rb3[j]) for j in range(n)]
    arrived = [
        jnp.concatenate([blk[sl * q : sl * q + sl, :] for blk in blocks], axis=0).astype(BF) for q in range(4)
    ]
    none = jnp.zeros((HEAD, STATE), BF)
    y_all = yacc[...]
    for d in range(2):
        top = jnp.concatenate([arrived[2 * d], none], axis=1)
        bottom = jnp.concatenate([none, arrived[2 * d + 1]], axis=1)
        into = dot_nt(mixed[:, 384:640], jnp.concatenate([top, bottom], axis=0))
        grow = jnp.where(low, turned[:, 16 + 2 * d : 17 + 2 * d], turned[:, 17 + 2 * d : 18 + 2 * d])
        y_all = y_all + into * grow
    g = y_all * silu(p2[EDGE : EDGE + length, 384:512])
    sq = g * g
    mean0 = jnp.sum(jnp.where(low, sq, 0.0), axis=-1, keepdims=True) / HEAD
    mean1 = jnp.sum(jnp.where(low, 0.0, sq), axis=-1, keepdims=True) / HEAD
    inv = jnp.where(low, lax.rsqrt(mean0 + EPS), lax.rsqrt(mean1 + EPS))
    ycat[:, 128:256] = (g * inv * wide(lane_ref[...])).astype(BF)

    def span(c):
        return slice(c * wcol, (c + 1) * wcol)

    def to_pair(c):
        return remote(
            obf.at[:, 1 - core, :, span(c)], prx.at[:, :, span(c)], os_.at[0], or_.at[c], z, y, cx * 2 + 1 - core
        )

    right = (cx + 1) % nx
    left = (cx + nx - 1) % nx
    opposite = (cx + 2) % nx

    def relay(c):
        xx = right if c < ncol // 2 else left
        return remote(
            xsend.at[opposite, :, span(c)], lrecv.at[:, span(c)], xs.at[0], xr.at[0, c], z, y, xx * 2 + core
        )

    def to_owner(c, side):
        xx = (right, left)[side]
        return remote(
            xsend.at[xx, :, span(c)], xrecv.at[side, :, span(c)], xs.at[1], xr.at[1, c], z, y, xx * 2 + core
        )

    def owner_in(c):
        ref = xrecv.at[:, :, span(c)]
        remote(ref, ref, xs.at[1], xr.at[1, c], z, y, tp).wait_recv()

    def chip_sum(xx, c):
        return wide(obf[xx, core, :, span(c)]) + wide(prx[xx, :, span(c)])

    order = [c for pair in zip(range(ncol // 2), range(ncol // 2, ncol)) for c in pair]
    exits = w2[:, :, :, :, 512:768].reshape(dim, 2 * CH)
    for c in order:
        got = dot_nt(ycat[...], exits[c * wcol : (c + 1) * wcol, :])
        obf[:, :, :, span(c)] = got.astype(BF).reshape(nx, 2, rows, wcol)
        to_pair(c).start()
    for c in order:
        to_pair(c).wait_recv()
        xsend[opposite, :, span(c)] = chip_sum(opposite, c).astype(BF)
        relay(c).start()
    for c in order:
        side = 1 if c < ncol // 2 else 0
        xx = (right, left)[side]
        xsend[xx, :, span(c)] = chip_sum(xx, c).astype(BF)
        to_owner(c, side).start()
    for c in order:
        relay(c).wait_recv()
        side = 0 if c < ncol // 2 else 1
        xx = (right, left)[side]
        xsend[xx, :, span(c)] = (chip_sum(xx, c) + wide(lrecv[:, span(c)])).astype(BF)
        to_owner(c, side).start()
    drain1()
    drain2()
    for c in order:
        own = chip_sum(cx, c)
        owner_in(c)
        out_ref[:, span(c)] = (own + wide(xrecv[0, :, span(c)]) + wide(xrecv[1, :, span(c)])).astype(BF)

    remote(prx, prx, os_.at[0], or_.at[0], z, y, tp).wait_send()
    relayed = xsend.at[0]
    remote(relayed, relayed, xs.at[0], xr.at[0, 0], z, y, tp).wait_send()
    owned = xsend.at[0:2]
    remote(owned, owned, xs.at[1], xr.at[1, 0], z, y, tp).wait_send()
    for which in range(3):
        e_all(which).wait_send()
    a_wait(nx - 1, 0).wait_send()
    a_wait(nx, 1).wait_send()

    @pl.when((tp == far) & (sp < n * n - 1))
    def _():
        edge_next().wait_send()

    @pl.when((tp == 0) & (sp > 0))
    def _():
        edge_prev().wait_send()

    @pl.when((tp == far) & (sp > 0))
    def _():
        edge_sent(0)

    @pl.when((tp == 0) & (sp < n * n - 1))
    def _():
        edge_sent(1)


def half_way(nx):
    return nx // 2


def run_layer(n, tps, ncol, *args):
    (
        x,
        gain,
        slide,
        rec,
        lat,
        step,
        ctap,
        xtap,
        ltap,
        rate,
        spike,
        lane,
        cexit,
        sexit,
    ) = args
    rows, dim = x.shape
    length = rows * tps
    tall = length + 2 * EDGE
    nx = tps // 2
    half = n // 2
    sl = HEAD // n
    vm = pltpu.VMEM
    dma = pltpu.SemaphoreType.DMA
    vmem = pl.BlockSpec(memory_space=pltpu.VMEM)
    specs = [pl.BlockSpec(memory_space=pltpu.HBM)] * 14
    operands = (
        x,
        gain.reshape(dim // 128, 128),
        slide,
        rec,
        lat,
        step.transpose(1, 2, 0),
        ctap,
        xtap,
        ltap,
        rate,
        spike.T,
        lane.reshape(1, CH),
        cexit.T,
        sexit.T,
    )
    return pl.pallas_call(
        functools.partial(layer, n, tps),
        out_shape=pltpu.VMEM((rows, dim), BF),
        in_specs=specs,
        out_specs=vmem,
        scratch_shapes=[
            vm((tall, dim), BF),
            vm((n, n, 2, 16, 640), BF),
            vm((n, n, 2, 16, 768), BF),
            vm((tall, 640), F32),
            vm((tall, 512), F32),
            vm((length, 640), BF),
            vm((length, 256), BF),
            vm((length, 128), F32),
            vm((n, 4 * sl + 8, STATE), BF),
            vm((n, 4 * sl + 8, STATE), BF),
            vm((4 * sl + 8, STATE), BF),
            vm((n, 4 * sl + 8, STATE), BF),
            vm((n, 4 * sl, STATE), BF),
            vm((n, 4 * sl, STATE), BF),
            vm((n, 4 * sl, STATE), F32),
            vm((n, 8, STATE), F32),
            vm((nx, 2, rows, dim), BF),
            vm((nx, rows, dim), BF),
            vm((nx, rows, dim), BF),
            vm((2, rows, dim), BF),
            vm((rows, dim), BF),
            dma((1,)),
            dma((half, n)),
            dma((1,)),
            dma((half, n)),
            dma((2,)),
            dma((2, n)),
            dma((2,)),
            dma((1 + nx,)),
            dma((2, 2)),
            dma((2,)),
            dma((3,)),
            dma((3,)),
            dma((1,)),
            dma((ncol,)),
            dma((2,)),
            dma((2, ncol)),
            *[vm(v.shape, v.dtype) for v in operands],
            dma((14,)),
        ],
        compiler_params=pltpu.CompilerParams(
            collective_id=0, has_side_effects=True, vmem_limit_bytes=60 * 1024 * 1024
        ),
        name="layer",
    )(*operands)


def solution(mesh):
    n = 8 if mesh.shape["sp"] == 64 else int(round(mesh.shape["sp"] ** 0.5))
    sp_tp = ("sp", "tp")
    return jax.shard_map(
        functools.partial(run_layer, n, mesh.shape["tp"], 4),
        mesh=mesh,
        in_specs=(
            P(sp_tp, None),
            P(),
            P(None, "sp", "tp"),
            P(None, "sp", "tp"),
            P(None, "sp", "tp"),
            P(None, None, "tp"),
            P(None, "tp"),
            P(None, "tp"),
            P(None, None, "tp"),
            P(None, "tp"),
            P("sp", "tp"),
            P("tp"),
            P("tp", "sp"),
            P("tp", "sp"),
        ),
        out_specs=P(sp_tp, None),
        check_vma=False,
    )
```
